128 devices in a mesh: ep: 32 (over z, y, core), tp: 4 (over x).
Axes of the slice: x: 4, y: 4, z: 4, core: 2. Of those that a mesh axis runs over, the one named last changes fastest.
Arguments:
- tokens: bfloat16 [512, 2048], P('ep'), may hold values from -60 to 60
- mixer_gain: float32 [2048], replicated, may hold values from 0.1 to 1.9
- query_weight: bfloat16 [2048, 2048], P('ep', 'tp'), may hold values from -0.125 to 0.125
- key_weight: bfloat16 [2048, 2048], P('ep', 'tp'), may hold values from -0.125 to 0.125
- value_weight: bfloat16 [2048, 2048], P('ep', 'tp'), may hold values from -0.125 to 0.125
- outgate_weight: bfloat16 [2048, 2048], P('ep', 'tp'), may hold values from -0.125 to 0.125
- igate_weight: bfloat16 [4, 2048], P('tp'), may hold values from -0.125 to 0.125
- fgate_weight: bfloat16 [4, 2048], P('tp'), may hold values from -0.125 to 0.125
- memory: float32 [512, 4, 512, 512], P('ep', 'tp'), may hold values from -6 to 6
- stabilizer: float32 [512, 4], P('ep', 'tp'), may hold values from -6 to 6
- head_gain: float32 [2048], P('tp'), may hold values from 0.1 to 1.9
- down_weight: bfloat16 [2048, 2048], P(None, 'ep'), may hold values from -1 to 1
- mixed_gain: float32 [2048], P('ep'), may hold values from 0.1 to 1.9
- expert_gain: float32 [2048], P('ep'), may hold values from 0.1 to 1.9
- routes: int32 [512, 4], replicated, may hold values from 0 to 31, all different within a row; in each aligned block of 16 rows (0 to 15, 16 to 31, ...) at most 4 rows name the same one
- route_weights: float32 [512, 4], replicated, may hold values from 0.1 to 1
- gate_proj: bfloat16 [32, 2048, 2048], P('ep', None, 'tp'), may hold values from -0.5 to 0.5
- up_proj: bfloat16 [32, 2048, 2048], P('ep', None, 'tp'), may hold values from -0.5 to 0.5
- expert_down: bfloat16 [32, 2048, 2048], P('ep', 'tp'), may hold values from -1 to 1
- output_gain: float32 [2048], P('tp'), may hold values from 0.1 to 1.9
Outputs:
- layer_out: bfloat16 [512, 2048], P('ep', 'tp')
The draws below stay inside these ranges and needn't reach their ends.
Inputs may be any that keep to these rules, and one draw needn't show every extreme that they name: `routes`: each row names 4 different experts; within the rows of one device (16 rows) no expert is named more than 4 times, a bound that some block reaches.
All inputs are finite; a program needn't handle non-finite values.
Results may differ from the reference program's by a relative error of at most 0.0095.
Values may be sent and summed in bfloat16 or wider, within the bound.
No kernel may reach another device: no remote copies, remote signals or barrier semaphores. Data moves between devices by JAX's collectives and lax.ppermute only.
A program may use at most 128 MiB of HBM per device.

```python
import math
import jax
import jax.numpy as jnp
import numpy as np
from jax import lax

D = 2048
HEADS = 4
DH = 512
DE = 2048
TOP_K = 4
SEQ_DEV = 16
TOKENS = 512
EXPERTS = 32
CAP = 4
N_EP = 32


def column_ramp(key, width, spread):
    rough = jax.random.uniform(key, (width,), jnp.float32, -0.3, 0.3)
    return jnp.exp(jnp.linspace(-spread, spread, width) + rough)


def draw_tokens(key, part):
    base = jax.random.normal(jax.random.fold_in(key, 11), (TOKENS, D), jnp.float32)
    row_scale = jnp.exp(jax.random.uniform(jax.random.fold_in(key, 12), (TOKENS, 1), jnp.float32, jnp.log(0.4), jnp.log(4.0)))
    ramp = column_ramp(jax.random.fold_in(key, 14), D, 0.55)
    values = base * row_scale * ramp[None, :]
    return jnp.clip(values, -60.0, 60.0).astype(jnp.bfloat16)


def draw_down_weight(key, part):
    base = jax.random.normal(jax.random.fold_in(key, 21), (HEADS * DH, D), jnp.float32) / jnp.sqrt(HEADS * DH * 1.0)
    ramp = column_ramp(jax.random.fold_in(key, 22), D, 0.55)
    return jnp.clip(base * ramp[None, :], -1.0, 1.0).astype(jnp.bfloat16)


def draw_expert_down(key, part):
    base = jax.random.normal(jax.random.fold_in(key, 31), (EXPERTS, DE, D), jnp.float32) / jnp.sqrt(DE * 1.0)
    ramp = column_ramp(jax.random.fold_in(key, 32), D, 0.55)
    return jnp.clip(base * ramp[None, None, :], -1.0, 1.0).astype(jnp.bfloat16)


def level_of(own_key, shape, shards, low, high):
    def one(dim, parts):
        draws = jax.random.uniform(jax.random.fold_in(jax.random.fold_in(own_key, 6), dim), (parts,), jnp.float32, low / len(shards), high / len(shards))
        return jnp.repeat(jnp.exp(draws), shape[dim] // parts).reshape((-1,) + (1,) * (len(shape) - dim - 1))

    loudness = one(*shards[0])
    for cut in shards[1:]:
        loudness = loudness * one(*cut)
    return loudness


def assign_block(stream_key, own, number, rows, amount, top, bound, skew):
    order = jax.random.permutation(stream_key, amount)
    crowded, usual = load_shares(amount, rows * top, bound, skew, True), load_shares(amount, rows * top, bound, skew, False)
    places = jnp.arange(amount)

    def named(lengths, rotation):
        used = int((lengths > 0).sum())
        fixed = max(1, used // 4)
        passed = fixed + (places - fixed + rotation * (used - fixed)) % max(1, amount - fixed)
        return jnp.zeros((amount,), jnp.int32).at[order[jnp.where(places < fixed, places, passed)]].set(jnp.asarray(lengths, jnp.int32))

    lengths = jnp.where(number % 4 == 0, named(crowded, number // 4), named(usual, number - number // 4 - 1))
    mixed = jax.random.permutation(jax.random.fold_in(own, 3), amount)
    donor, sink = mixed[0:amount // 2 * 2:2], mixed[1:amount // 2 * 2:2]
    slack = jnp.minimum(lengths[donor] - 1, bound - lengths[sink]) // 2
    slack = jnp.where((donor == order[0]) | (sink == order[0]) | (lengths[sink] == 0), 0, jnp.maximum(slack, 0))
    passed = jax.random.randint(jax.random.fold_in(own, 4), (amount // 2,), 0, 1 << 20) % (slack + 1)
    lengths = lengths.at[donor].add(-passed).at[sink].add(passed)
    members = jnp.searchsorted(jnp.cumsum(lengths), jnp.arange(rows * top), side="right").astype(jnp.int32)
    table = members.reshape(top, rows).T
    table = table[jax.random.permutation(jax.random.fold_in(own, 1), rows)]
    rotation = jax.random.randint(jax.random.fold_in(own, 2), (rows, 1), 0, top)
    return jnp.take_along_axis(table, (jnp.arange(top)[None, :] + rotation) % top, axis=1)


def load_shares(count, total, most, lean, full):
    loads = [(1 << 20) // math.isqrt(standing ** lean) + 1 for standing in range(1, count + 1)]
    largest = most if full else min(most, max(-(-total // count), total * loads[0] // sum(loads)))
    least = 1 if total - largest >= count - 1 else 0
    given, surplus = [largest] + [least] * (count - 1), total - largest - least * (count - 1)
    while surplus > 0:
        free = [i for i in range(1, count) if given[i] < largest] or [i for i in range(1, count) if given[i] < most]
        mass, budget = sum([loads[i] for i in free]), surplus
        for i in free:
            extra = min(most - given[i], max(1, budget * loads[i] // mass), surplus)
            given[i] = given[i] + extra
            surplus = surplus - extra
    return np.array(given)


def centred(key, shape, scale, reach, cuts=(), held_as=jnp.bfloat16):
    loudness = level_of(key, shape, cuts, -0.22, 0.18) if cuts else 1.0
    drawn = jax.random.normal(key, shape, jnp.float32) * scale * loudness
    return jnp.minimum(jnp.maximum(drawn, -reach), reach).astype(held_as)


def setup_inputs(seed: int = 0) -> dict:
    streams_of = jax.random.split(jax.random.key(seed), 21)
    tokens = draw_tokens(jax.random.fold_in(streams_of[20], 71), 0)
    mixer_gain = jnp.clip(1.0 + 0.18 * jax.random.normal(streams_of[1], (D,), jnp.float32), 0.1, 1.9)
    query_weight = centred(streams_of[2], (D, HEADS * DH), D ** -0.5, 0.125, ((0, 32), (1, 4)))
    key_weight = centred(streams_of[3], (D, HEADS * DH), D ** -0.5, 0.125, ((0, 32), (1, 4)))
    value_weight = centred(streams_of[4], (D, HEADS * DH), D ** -0.5, 0.125, ((0, 32), (1, 4)))
    outgate_weight = centred(streams_of[5], (D, HEADS * DH), D ** -0.5, 0.125, ((0, 32), (1, 4)))
    igate_weight = centred(streams_of[6], (HEADS, D), D ** -0.5, 0.125, ((0, 4),))
    fgate_weight = centred(streams_of[7], (HEADS, D), D ** -0.5, 0.125, ((0, 4),))
    memory = centred(streams_of[8], (TOKENS, HEADS, DH, DH), 1.0, 6.0, ((0, 32), (1, 4)), jnp.float32)
    stabilizer = centred(streams_of[9], (TOKENS, HEADS), 1.5, 6.0, ((0, 32), (1, 4)), jnp.float32)
    head_gain = jnp.clip(1.0 + 0.18 * jax.random.normal(streams_of[10], (HEADS * DH,), jnp.float32), 0.1, 1.9)
    down_weight = draw_down_weight(jax.random.fold_in(streams_of[20], 71), 0)
    mixed_gain = jnp.clip(1.0 + 0.18 * jax.random.normal(streams_of[12], (D,), jnp.float32), 0.1, 1.9)
    expert_gain = jnp.clip(1.0 + 0.18 * jax.random.normal(streams_of[13], (D,), jnp.float32), 0.1, 1.9)
    routes_keys = jax.random.split(jax.random.fold_in(streams_of[14], 1), TOKENS // SEQ_DEV)
    routes_turns = jax.random.permutation(jax.random.fold_in(streams_of[14], 3), TOKENS // SEQ_DEV)
    routes = jax.vmap(lambda own, number: assign_block(jax.random.fold_in(streams_of[14], 2), own, number, SEQ_DEV, EXPERTS, TOP_K, CAP, 2))(routes_keys, routes_turns).reshape((TOKENS, TOP_K))
    route_weights = jnp.clip(jax.random.uniform(streams_of[15], (TOKENS, TOP_K), jnp.float32, 0.1, 1.0), 0.1, 1.0)
    gate_proj = centred(streams_of[16], (EXPERTS, D, DE), (D // 16) ** -0.5, 0.5, ((0, 32), (2, 4)))
    up_proj = centred(streams_of[17], (EXPERTS, D, DE), (D // 16) ** -0.5, 0.5, ((0, 32), (2, 4)))
    expert_down = draw_expert_down(jax.random.fold_in(streams_of[20], 71), 0)
    output_gain = jnp.clip(1.0 + 0.18 * jax.random.normal(streams_of[19], (D,), jnp.float32), 0.1, 1.9)
    return dict(tokens=tokens, mixer_gain=mixer_gain, query_weight=query_weight, key_weight=key_weight, value_weight=value_weight, outgate_weight=outgate_weight, igate_weight=igate_weight, fgate_weight=fgate_weight, memory=memory, stabilizer=stabilizer, head_gain=head_gain, down_weight=down_weight, mixed_gain=mixed_gain, expert_gain=expert_gain, routes=routes, route_weights=route_weights, gate_proj=gate_proj, up_proj=up_proj, expert_down=expert_down, output_gain=output_gain)


NORM_EPS = 1e-06
CLAMP_LIMIT = 7.0
SIGMOID_SCALE = 1.702

def rms_scale(values):
    return lax.rsqrt(lax.optimization_barrier(jnp.mean(values * values, axis=-1, keepdims=True)) + NORM_EPS)

def slot_tables(routes, groups, experts, capacity):
    token_total, top_count = routes.shape
    per_group = token_total // groups
    flat_routes = routes.reshape(groups, per_group * top_count)
    onehot = (flat_routes[:, :, None] == jnp.arange(experts, dtype=jnp.int32)[None, None, :]).astype(jnp.int32)
    before = jnp.cumsum(onehot, axis=1) - onehot
    slot_index = lax.optimization_barrier(jnp.sum(before * onehot, axis=2))
    group_ids = jnp.arange(groups, dtype=jnp.int32)[:, None]
    destination = ((flat_routes * groups + group_ids) * capacity + slot_index).reshape(token_total, top_count)
    owner_token = jnp.arange(token_total * top_count, dtype=jnp.int32) // top_count
    slot_token = jnp.full((experts * groups * capacity,), token_total, jnp.int32).at[destination.reshape(-1)].set(owner_token)
    return (destination, slot_token)

def read_memory(projected, log_input, log_forget, memory, stabilizer, head_gain):
    row_total, head_count, head_size = (memory.shape[0], memory.shape[1], memory.shape[3])
    query_scaled = projected[:, 0] * head_size ** (-0.5)
    key_rows = projected[:, 1]
    value_rows = projected[:, 2]
    outgate_rows = projected[:, 3]
    peak_log = jnp.maximum(log_forget + stabilizer, log_input)
    within = jnp.exp(log_input - peak_log)
    carried = jnp.exp(log_forget + stabilizer - peak_log)
    scores = lax.optimization_barrier(jnp.sum(query_scaled * key_rows, axis=-1)) * within
    state_read = jnp.einsum('nhd,nhde->nhe', query_scaled, memory, precision=lax.Precision.HIGHEST)
    read_value = scores[..., None] * value_rows + carried[..., None] * state_read
    head_mean = lax.optimization_barrier(jnp.mean(read_value, axis=-1, keepdims=True))
    centered = read_value - head_mean
    head_var = lax.optimization_barrier(jnp.mean(centered * centered, axis=-1, keepdims=True))
    normalized = centered * lax.rsqrt(head_var + NORM_EPS)
    gained = normalized * head_gain.reshape(head_count, head_size) * jax.nn.sigmoid(outgate_rows)
    return gained.reshape(row_total, head_count * head_size).astype(jnp.bfloat16)

def apply_expert(arguments):
    row_block, gate_matrix, up_matrix, down_matrix = arguments
    gate_pre = jnp.minimum(jnp.dot(row_block, gate_matrix, preferred_element_type=jnp.float32), CLAMP_LIMIT)
    up_pre = jnp.clip(jnp.dot(row_block, up_matrix, preferred_element_type=jnp.float32), -CLAMP_LIMIT, CLAMP_LIMIT)
    activation = ((up_pre + 1.0) * gate_pre * jax.nn.sigmoid(SIGMOID_SCALE * gate_pre)).astype(jnp.bfloat16)
    return jnp.dot(activation, down_matrix, preferred_element_type=jnp.float32)

def reference(tokens, mixer_gain, query_weight, key_weight, value_weight, outgate_weight, igate_weight, fgate_weight, memory, stabilizer, head_gain, down_weight, mixed_gain, expert_gain, routes, route_weights, gate_proj, up_proj, expert_down, output_gain):
    tokens_float = tokens.astype(jnp.float32)
    normed = (tokens_float * rms_scale(tokens_float) * mixer_gain).astype(jnp.bfloat16)
    projected = jnp.concatenate([jnp.dot(normed, matrix, preferred_element_type=jnp.float32) for matrix in (query_weight, key_weight, value_weight, outgate_weight)], axis=1).astype(jnp.bfloat16)
    projected = lax.optimization_barrier(projected).astype(jnp.float32).reshape(TOKENS, 4, HEADS, DH)
    log_input = jnp.dot(normed, igate_weight.T, preferred_element_type=jnp.float32)
    log_forget = jax.nn.log_sigmoid(jnp.dot(normed, fgate_weight.T, preferred_element_type=jnp.float32))
    gated_heads = read_memory(projected, log_input, log_forget, memory, stabilizer, head_gain)
    mixed_rows = jnp.dot(gated_heads, down_weight, preferred_element_type=jnp.float32)
    residual_float = tokens_float + mixed_rows * rms_scale(mixed_rows) * mixed_gain
    residual = residual_float.astype(jnp.bfloat16)
    expert_in = (residual_float * rms_scale(residual_float) * expert_gain).astype(jnp.bfloat16)
    destination, slot_token = slot_tables(routes, N_EP, EXPERTS, CAP)
    padded_in = jnp.concatenate([expert_in, jnp.zeros((1, D), jnp.bfloat16)], axis=0)
    expert_inputs = padded_in[slot_token].reshape(EXPERTS, N_EP * CAP, D)
    expert_out = lax.map(apply_expert, (expert_inputs, gate_proj, up_proj, expert_down))
    picked = expert_out.reshape(EXPERTS * N_EP * CAP, D)[destination]
    combined = lax.optimization_barrier(jnp.sum(picked * route_weights[..., None], axis=1))
    final_rows = residual.astype(jnp.float32) + combined * rms_scale(combined) * output_gain
    return final_rows.astype(jnp.bfloat16)
```

```python
import jax
import jax.numpy as jnp
from jax import lax
from jax.experimental import pallas as pl
from jax.experimental.pallas import tpu as pltpu
from jax.sharding import PartitionSpec as P

NORM_EPS = 1e-06
CLAMP_LIMIT = 7.0
SIGMOID_SCALE = 1.702
BF = jnp.bfloat16
F32 = jnp.float32
Z, Y, C, TP = 4, 4, 2, 4
CAP = 4


def ep_at(z, y, c):
    return (z % Z) * (Y * C) + (y % Y) * C + c % C


def ep_moves(dz, dy, dc):
    return [
        (ep_at(z, y, c), ep_at(z + dz, y + dy, c + dc))
        for z in range(Z)
        for y in range(Y)
        for c in range(C)
    ]


def along_z(a, s):
    return lax.ppermute(a, "ep", ep_moves(s, 0, 0))


def along_y(a, s):
    return lax.ppermute(a, "ep", ep_moves(0, s, 0))


def other_core(a):
    return lax.ppermute(a, "ep", ep_moves(0, 0, 1))


def along_tp(a, s):
    return lax.ppermute(a, "tp", [(i, (i + s) % TP) for i in range(TP)])


def rms_scale(values):
    return lax.rsqrt(jnp.mean(values * values, axis=-1, keepdims=True) + NORM_EPS)


def project_kernel(at, n0, n1, n2, n3, w0, w1, w2, w3, p0, p1, p2, p3, own, t1, t2, t3):
    z, y, c = at[0], at[1], at[2]
    rows = []
    for n in (n0, n1, n2, n3):
        chunks = []
        for s in range(Z):
            off = pl.multiple_of(((z + (Z - s)) & 3) * 512 + y * 128, 128)
            part = n[:, pl.ds(off, 128)].astype(F32)
            chunks.append(jnp.where(c == 0, part, pltpu.roll(part, 64, 1)).astype(BF))
        rows.append(jnp.concatenate(chunks, axis=1))
    x = jnp.concatenate(rows, axis=0)
    w = jnp.concatenate(
        [r[...] for pair in zip((w0, w1, w2, w3), (p0, p1, p2, p3)) for r in pair], axis=0
    )
    acc = jnp.dot(x, w, preferred_element_type=F32)
    i = pl.program_id(0)
    own[...] = acc[0:16]
    for k, t in ((16, t1), (32, t2), (48, t3)):
        part = acc[k : k + 16]
        high = part.astype(BF)
        t[:, pl.ds(pl.multiple_of(i * 512, 128), 512)] = high

        @pl.when(i < 2)
        def _():
            low = (part - high.astype(F32)).astype(BF)
            t[:, pl.ds(pl.multiple_of(2048 + i * 512, 128), 512)] = low


def project(at, normed_by_shift, weights, partner):
    rows, width = normed_by_shift[0].shape
    whole = pl.BlockSpec((rows, width), lambda i: (0, 0))
    wide = pl.BlockSpec((64, 512), lambda i: (0, i))
    sent = width + width // 2
    return pl.pallas_call(
        project_kernel,
        grid=(4,),
        in_specs=[pl.BlockSpec(memory_space=pltpu.SMEM)] + [whole] * 4 + [wide] * 8,
        out_specs=[pl.BlockSpec((rows, 512), lambda i: (0, i))]
        + [pl.BlockSpec((rows, sent), lambda i: (0, 0))] * 3,
        out_shape=[jax.ShapeDtypeStruct((rows, width), F32)]
        + [jax.ShapeDtypeStruct((rows, sent), BF)] * 3,
        name="project",
    )(at, *normed_by_shift, *weights, *partner)


def down_kernel(at, g, d0, d1, d2, d3, e0, e1, e2, e3, part, send, gains, full):
    z, y, c = at[0], at[1], at[2]
    lane = lax.broadcasted_iota(jnp.int32, (16, 128), 1)
    row = lax.broadcasted_iota(jnp.int32, (16, 128), 0)
    eye = jnp.where(lane == row, 1.0, 0.0).astype(BF)
    a = jnp.concatenate(
        [
            jnp.concatenate([g[...], jnp.zeros((16, 128), BF)], axis=1),
            jnp.concatenate([jnp.zeros((16, 512), BF), eye], axis=1),
        ],
        axis=0,
    )
    low = lax.broadcasted_iota(jnp.int32, (32, 128), 1) < 64
    for s, (d, e) in enumerate(zip((d0, d1, d2, d3), (e0, e1, e2, e3))):
        mine = lax.dot_general(a, d[...], (((1,), (1,)), ((), ())), preferred_element_type=F32)
        other = lax.dot_general(a, e[...], (((1,), (1,)), ((), ())), preferred_element_type=F32)
        for t in range(Y):
            j = t // 2 * 128
            m, o = mine[:, j : j + 128], other[:, j : j + 128]
            first = jnp.where(c == 0, m, o)
            second = jnp.where(c == 0, o, m)
            if t % 2 == 0:
                block = jnp.where(low, first, pltpu.roll(second, 64, 1))
            else:
                block = jnp.where(low, pltpu.roll(first, 64, 1), second)
            off = pl.multiple_of(((z + (Z - s)) & 3) * 512 + ((y + (Y - t)) & 3) * 128, 128)
            full[:, pl.ds(off, 128)] = block
    part[...] = full[0:16]
    send[...] = full[0:16].astype(BF)
    mixed_gain = full[16:17] + full[17:18] + full[18:19]
    expert_gain = full[19:20] + full[20:21] + full[21:22]
    gains[...] = jnp.concatenate(
        [mixed_gain, expert_gain, jnp.zeros((6, mixed_gain.shape[1]), F32)], axis=0
    )


def down_project(at, gated, own, partner):
    rows = gated.shape[0]
    vmem = pl.BlockSpec(memory_space=pltpu.VMEM)
    return pl.pallas_call(
        down_kernel,
        in_specs=[pl.BlockSpec(memory_space=pltpu.SMEM)] + [vmem] * 9,
        out_specs=[vmem] * 3,
        out_shape=[
            jax.ShapeDtypeStruct((rows, 2048), F32),
            jax.ShapeDtypeStruct((rows, 2048), BF),
            jax.ShapeDtypeStruct((8, 2048), F32),
        ],
        scratch_shapes=[pltpu.VMEM((32, 2048), F32)],
        name="down_project",
    )(at, gated, *own, *partner)


def in_three(values):
    high = lax.reduce_precision(values, 8, 7)
    rest = values - high
    mid = lax.reduce_precision(rest, 8, 7)
    return [v.astype(BF) for v in (high, mid, rest - mid)]


def read_memory(projected, log_input, log_forget, memory, stabilizer, head_gain):
    row_total, head_count, head_size = (memory.shape[0], memory.shape[1], memory.shape[3])
    query_scaled = projected[:, 0] * head_size ** (-0.5)
    key_rows = projected[:, 1]
    value_rows = projected[:, 2]
    outgate_rows = projected[:, 3]
    peak_log = jnp.maximum(log_forget + stabilizer, log_input)
    within = jnp.exp(log_input - peak_log)
    carried = jnp.exp(log_forget + stabilizer - peak_log)
    scores = jnp.sum(query_scaled * key_rows, axis=-1) * within
    state_read = jnp.einsum("nhd,nhde->nhe", query_scaled, memory)
    read_value = scores[..., None] * value_rows + carried[..., None] * state_read
    head_mean = jnp.mean(read_value, axis=-1, keepdims=True)
    centered = read_value - head_mean
    head_var = jnp.mean(centered * centered, axis=-1, keepdims=True)
    normalized = centered * lax.rsqrt(head_var + NORM_EPS)
    gained = normalized * head_gain.reshape(head_count, head_size) * jax.nn.sigmoid(outgate_rows)
    return gained.reshape(row_total, head_count * head_size).astype(BF)


def shards(
    tokens,
    mixer_gain,
    query_weight,
    key_weight,
    value_weight,
    outgate_weight,
    igate_weight,
    fgate_weight,
    memory,
    stabilizer,
    head_gain,
    down_weight,
    mixed_gain,
    expert_gain,
    routes,
    route_weights,
    gate_proj,
    up_proj,
    expert_down,
    output_gain,
):
    ep_count = lax.axis_size("ep")
    ep_index = lax.axis_index("ep")
    tp_index = lax.axis_index("tp")
    at = jnp.stack([ep_index // (Y * C), ep_index // C % Y, ep_index % C]).astype(jnp.int32)
    own_rows, width = tokens.shape
    tp_width = output_gain.shape[0]
    head_rows = memory.shape[3]

    with jax.named_scope("weights"):
        w0 = jnp.concatenate([query_weight, key_weight, value_weight, outgate_weight], axis=1)
        by_z = [w0] + [along_z(w0, s) for s in (1, 2, 3)]
        partner = [other_core(w) for w in by_z]

    with jax.named_scope("tokens"):
        tokens_float = tokens.astype(F32)
        normed = (tokens_float * rms_scale(tokens_float) * mixer_gain).astype(BF)
        by_y = [normed] + [along_y(normed, s) for s in (1, 2, 3)]
        log_input = jnp.einsum("sd,hd->sh", normed, igate_weight, preferred_element_type=F32)
        log_forget = jax.nn.log_sigmoid(
            jnp.einsum("sd,hd->sh", normed, fgate_weight, preferred_element_type=F32)
        )

    with jax.named_scope("down"):
        rows_of_head = lax.dynamic_slice_in_dim(down_weight, tp_index * head_rows, head_rows, 0)
        extra = jnp.stack(in_three(mixed_gain) + in_three(expert_gain), axis=1)
        extra = jnp.pad(extra, ((0, 0), (0, 128 - extra.shape[1])))
        d0 = jnp.concatenate([rows_of_head.T, extra], axis=1)
        down_y = jnp.concatenate([d0] + [along_y(d0, s) for s in (1, 2, 3)], axis=0)
        down_z = [down_y] + [along_z(down_y, s) for s in (1, 2, 3)]
        down_partner = [other_core(d) for d in down_z]

    with jax.named_scope("routing"):
        my_routes = lax.dynamic_slice_in_dim(routes, ep_index * own_rows, own_rows, 0)
        my_weights = lax.dynamic_slice_in_dim(route_weights, ep_index * own_rows, own_rows, 0)
        experts = jnp.arange(ep_count, dtype=jnp.int32)
        hit = my_routes[:, :, None] == experts[None, None, :]
        named = jnp.any(hit, axis=1)
        weight_of = jnp.sum(jnp.where(hit, my_weights[:, :, None], 0.0), axis=1)
        earlier = jnp.arange(own_rows)[:, None] > jnp.arange(own_rows)[None, :]
        slot = jnp.sum(
            jnp.where(earlier[:, :, None] & named[None, :, :], 1, 0), axis=1, dtype=jnp.int32
        )
        slots = jnp.arange(CAP, dtype=jnp.int32)
        placed = named[:, :, None] & (slot[:, :, None] == slots[None, None, :])
        send_from = placed.reshape(own_rows, ep_count * CAP)
        take_with = jnp.where(placed, weight_of[:, :, None], 0.0).reshape(
            own_rows, ep_count * CAP
        )

    with jax.named_scope("project"):
        own, t1, t2, t3 = project(at, by_y, by_z, partner)
        projected = own
        for s, t in ((1, t1), (2, t2), (3, t3)):
            came = along_y(t, -s).astype(F32)
            low = jnp.pad(came[:, width:], ((0, 0), (0, width // 2)))
            projected = projected + (came[:, :width] + low)
        projected = lax.reduce_precision(projected, 8, 7).reshape(own_rows, 4, 1, head_rows)

    with jax.named_scope("read"):
        gated = read_memory(projected, log_input, log_forget, memory, stabilizer, head_gain)
        part, send, gains = down_project(at, gated, down_z, down_partner)
        mixed = part
        for s in (1, 2, 3):
            mixed = mixed + along_tp(send, s).astype(F32)

    with jax.named_scope("dispatch"):
        residual_float = tokens_float + mixed * rms_scale(mixed) * gains[0]
        residual = lax.dynamic_slice_in_dim(
            residual_float.astype(BF), tp_index * tp_width, tp_width, 1
        )
        expert_in = (residual_float * rms_scale(residual_float) * gains[1]).astype(BF)
        outgoing = lax.dot_general(
            send_from.astype(BF), expert_in, (((0,), (0,)), ((), ())), preferred_element_type=F32
        ).astype(BF)
        arrived = lax.all_to_all(
            outgoing.reshape(ep_count, CAP, width), "ep", 0, 0, tiled=True
        ).reshape(ep_count * CAP, width)

    with jax.named_scope("experts"):
        gate_pre = jnp.minimum(
            jnp.dot(arrived, gate_proj[0], preferred_element_type=F32), CLAMP_LIMIT
        )
        up_pre = jnp.clip(
            jnp.dot(arrived, up_proj[0], preferred_element_type=F32), -CLAMP_LIMIT, CLAMP_LIMIT
        )
        activation = (
            (up_pre + 1.0) * gate_pre * jax.nn.sigmoid(SIGMOID_SCALE * gate_pre)
        ).astype(BF)
        partial_value = jnp.dot(activation, expert_down[0], preferred_element_type=F32)
        returned = lax.all_to_all(
            partial_value.astype(BF).reshape(ep_count, CAP, width), "ep", 0, 0, tiled=True
        ).reshape(ep_count * CAP, width)

    with jax.named_scope("combine"):
        partial = jnp.dot(
            take_with, returned.astype(F32), precision=lax.Precision.HIGHEST,
            preferred_element_type=F32,
        )
        partial_sent = partial.astype(BF)
        combined = partial
        for s in (1, 2, 3):
            combined = combined + along_tp(partial_sent, s).astype(F32)
        scale = rms_scale(combined)
        combined_mine = lax.dynamic_slice_in_dim(combined, tp_index * tp_width, tp_width, 1)
        final_rows = residual.astype(F32) + combined_mine * scale * output_gain
        return final_rows.astype(BF)


def solution(mesh):
    placed = (
        P("ep", None),
        P(),
        P("ep", "tp"),
        P("ep", "tp"),
        P("ep", "tp"),
        P("ep", "tp"),
        P("tp", None),
        P("tp", None),
        P("ep", "tp", None, None),
        P("ep", "tp"),
        P("tp"),
        P(None, "ep"),
        P("ep"),
        P("ep"),
        P(),
        P(),
        P("ep", None, "tp"),
        P("ep", None, "tp"),
        P("ep", "tp", None),
        P("tp"),
    )
    return jax.shard_map(
        shards, mesh=mesh, in_specs=placed, out_specs=P("ep", "tp"), check_vma=False
    )
```

```python
import jax
import jax.numpy as jnp
from jax import lax
from jax.experimental import pallas as pl
from jax.experimental.pallas import tpu as pltpu
from jax.sharding import PartitionSpec as P


NORM_EPS = 1e-06
CLAMP_LIMIT = 7.0
SIGMOID_SCALE = 1.702
BF = jnp.bfloat16
F32 = jnp.float32
Z, Y, C, TP = 4, 4, 2, 4
CAP = 4


def ep_at(z, y, c):
    return (z % Z) * (Y * C) + (y % Y) * C + c % C


def ep_moves(dz, dy, dc):
    return [
        (ep_at(z, y, c), ep_at(z + dz, y + dy, c + dc))
        for z in range(Z)
        for y in range(Y)
        for c in range(C)
    ]


def along_z(a, s):
    return lax.ppermute(a, "ep", ep_moves(s, 0, 0))


def along_y(a, s):
    return lax.ppermute(a, "ep", ep_moves(0, s, 0))


def other_core(a):
    return lax.ppermute(a, "ep", ep_moves(0, 0, 1))


def along_tp(a, s):
    return lax.ppermute(a, "tp", [(i, (i + s) % TP) for i in range(TP)])


def on_chip(*arrays):
    return [pltpu.with_memory_space_constraint(a, pltpu.VMEM) for a in arrays]


def kernel_room(mebibytes):
    return pltpu.CompilerParams(vmem_limit_bytes=mebibytes << 20)


def rms_scale(values):
    return lax.rsqrt(jnp.mean(values * values, axis=-1, keepdims=True) + NORM_EPS)


def join_kernel(q, k, v, o, w0, sems):
    loads = [
        pltpu.make_async_copy(r, w0.at[:, pl.ds(i * 512, 512)], sems.at[i])
        for i, r in enumerate((q, k, v, o))
    ]
    for load in loads:
        load.start()
    for load in loads:
        load.wait()


def join(weights):
    return pl.pallas_call(
        join_kernel,
        in_specs=[pl.BlockSpec(memory_space=pl.ANY)] * 4,
        out_specs=pl.BlockSpec(memory_space=pltpu.VMEM),
        out_shape=pltpu.VMEM((64, 2048), BF),
        scratch_shapes=[pltpu.SemaphoreType.DMA((4,))],
        name="join",
    )(*weights)


def prepare_kernel(
    at, x, gain, ig, fg, dw, mg, eg, stab, routes, weights, packed, gates, send, take
):
    xf = x[...].astype(F32)
    normed = (xf * rms_scale(xf) * gain[...]).astype(BF)
    for i in range(Z):
        packed[16 * i : 16 * i + 16, 640:1152] = normed[:, 512 * i : 512 * (i + 1)]
    nf = normed.astype(F32)
    log_input = jnp.sum(nf * ig[...].astype(F32), axis=1, keepdims=True)
    pre = jnp.sum(nf * fg[...].astype(F32), axis=1, keepdims=True)
    log_forget = jnp.minimum(pre, 0.0) - jnp.log1p(jnp.exp(-jnp.abs(pre)))
    small = lax.broadcasted_iota(jnp.int32, (16, 16), 0)
    across = lax.broadcasted_iota(jnp.int32, (16, 16), 1)
    stab_column = jnp.sum(jnp.where(small == across, stab[...], 0.0), axis=1, keepdims=True)
    lane = lax.broadcasted_iota(jnp.int32, (16, 128), 1)
    gates[...] = jnp.where(lane == 0, log_input, log_forget + stab_column)
    row = lax.broadcasted_iota(jnp.int32, (128, 64), 0)
    extra = jnp.zeros((128, 64), F32)
    for i, g in enumerate((mg, eg)):
        whole = g[...]
        high = whole.astype(BF).astype(F32)
        rest = whole - high
        mid = rest.astype(BF).astype(F32)
        for j, piece in enumerate((high, mid, rest - mid)):
            extra = jnp.where(row == 3 * i + j, piece, extra)
    eye = jnp.where(
        lax.broadcasted_iota(jnp.int32, (64, 64), 0) == lax.broadcasted_iota(jnp.int32, (64, 64), 1),
        1.0,
        0.0,
    ).astype(BF)
    turned = (((1,), (1,)), ((), ()))
    packed[:, 0:512] = dw[...]
    packed[:, 512:640] = lax.dot_general(
        eye, extra.astype(BF), turned, preferred_element_type=F32
    ).astype(BF)
    pick = jnp.where(
        lax.broadcasted_iota(jnp.int32, (16, 512), 1)
        == lax.broadcasted_iota(jnp.int32, (16, 512), 0) + at[1] * 16,
        1.0,
        0.0,
    )
    chosen = lax.dot_general(
        pick, routes[...].astype(F32), turned, precision=lax.Precision.HIGHEST,
        preferred_element_type=F32,
    )
    weight = lax.dot_general(
        pick, weights[...], turned, precision=lax.Precision.HIGHEST, preferred_element_type=F32
    )
    expert_of = (lane // CAP).astype(F32)
    named = jnp.zeros((16, 128), F32)
    weight_of = jnp.zeros((16, 128), F32)
    for k in range(4):
        hit = chosen[:, k : k + 1] == expert_of
        named = jnp.where(hit, 1.0, named)
        weight_of = jnp.where(hit, weight[:, k : k + 1], weight_of)
    before = jnp.dot(
        jnp.where(small > across, 1.0, 0.0).astype(BF), named.astype(BF),
        preferred_element_type=F32,
    )
    placed = (named > 0.5) & (before == (lane % CAP).astype(F32))
    send[...] = jnp.where(placed, 1.0, 0.0).astype(BF)
    take[...] = jnp.where(placed, weight_of, 0.0)


def prepare(at, tokens, mixer_gain, ig, fg, down_weight, mg, eg, stabilizer, routes, weights):
    def whole(a):
        return pl.BlockSpec(a.shape, lambda i, t: (0, 0))

    ins = [tokens, mixer_gain[None], ig, fg, down_weight.T, mg[None], eg[None]]
    ins += [stabilizer.T, routes.T, weights.T]
    specs = [whole(a) for a in ins]
    specs[4] = pl.BlockSpec((down_weight.shape[1], 512), lambda i, t: (0, t[0]))
    outs = [
        pltpu.VMEM((64, 1152), BF),
        pltpu.VMEM((16, 128), F32),
        pltpu.VMEM((16, 128), BF),
        pltpu.VMEM((16, 128), F32),
    ]
    return pl.pallas_call(
        prepare_kernel,
        grid_spec=pltpu.PrefetchScalarGridSpec(
            num_scalar_prefetch=1,
            grid=(1,),
            in_specs=specs,
            out_specs=[whole(a) for a in outs],
        ),
        out_shape=outs,
        name="prepare",
    )(at, *ins)


def project_kernel(
    at, n0, n1, n2, n3, w0, w1, w2, w3, p0, p1, p2, p3,
    own, t1, t2, t3,
):
    ep = at[1]
    z, y, c = ep // (Y * C), (ep // C) & 3, ep & 1
    col = pl.multiple_of(640 + y * 128, 128)
    rows = []
    for n in (n0, n1, n2, n3):
        chunks = []
        for s in range(Z):
            off = pl.multiple_of(((z + (Z - s)) & 3) * 16, 16)
            part = n[pl.ds(off, 16), pl.ds(col, 128)].astype(F32)
            chunks.append(jnp.where(c == 0, part, pltpu.roll(part, 64, 1)).astype(BF))
        rows.append(jnp.concatenate(chunks, axis=1))
    x = jnp.concatenate(rows, axis=0)
    pieces = [r for pair in zip((w0, w1, w2, w3), (p0, p1, p2, p3)) for r in pair]
    for i in range(4):
        at_i = slice(512 * i, 512 * (i + 1))
        w = jnp.concatenate([r[:, at_i] for r in pieces], axis=0)
        acc = jnp.dot(x, w, preferred_element_type=F32)
        own[:, at_i] = acc[0:16]
        for k, t in ((16, t1), (32, t2), (48, t3)):
            part = acc[k : k + 16]
            high = part.astype(BF)
            t[:, at_i] = high
            if i < 2:
                low = (part - high.astype(F32)).astype(BF)
                t[:, 2048 + 512 * i : 2048 + 512 * (i + 1)] = low


def project(at, packed_by_shift, weights, partner):
    rows, width = 16, weights[0].shape[1]
    vmem = pl.BlockSpec(memory_space=pltpu.VMEM)
    return pl.pallas_call(
        project_kernel,
        in_specs=[pl.BlockSpec(memory_space=pltpu.SMEM)] + [vmem] * 12,
        out_specs=[vmem] * 4,
        out_shape=[pltpu.VMEM((rows, width), F32)]
        + [pltpu.VMEM((rows, width + width // 2), BF)] * 3,
        compiler_params=kernel_room(8),
        name="project",
    )(at, *on_chip(*packed_by_shift, *weights, *partner))


def fetch_kernel(memory, out, sems):
    loads = [
        pltpu.make_async_copy(memory.at[n], out.at[n], sems.at[n]) for n in range(out.shape[0])
    ]
    for load in loads:
        load.start()
    for load in loads:
        load.wait()


def fetch(memory):
    return pl.pallas_call(
        fetch_kernel,
        in_specs=[pl.BlockSpec(memory_space=pltpu.HBM)],
        out_specs=pl.BlockSpec(memory_space=pltpu.VMEM),
        out_shape=pltpu.VMEM(memory.shape, F32),
        scratch_shapes=[pltpu.SemaphoreType.DMA((memory.shape[0],))],
        compiler_params=kernel_room(4),
        name="fetch",
    )(pltpu.with_memory_space_constraint(memory, pltpu.HBM))


def read_kernel(own, r1, r2, r3, gates, hg, mem, out):
    parts = []
    for i in range(4):
        at_i = slice(512 * i, 512 * (i + 1))
        total = own[:, at_i]
        for r in (r1, r2, r3):
            came = r[:, at_i].astype(F32)
            if i < 2:
                came = came + r[:, 2048 + 512 * i : 2048 + 512 * (i + 1)].astype(F32)
            total = total + came
        parts.append(total.astype(BF).astype(F32))
    query, key, value, outgate = parts
    query = query * 512 ** (-0.5)
    log_input, carry = gates[:, 0:1], gates[:, 1:2]
    peak = jnp.maximum(carry, log_input)
    within = jnp.exp(log_input - peak)
    carried = jnp.exp(carry - peak)
    score = jnp.sum(query * key, axis=1, keepdims=True) * within
    scaled = query * carried
    turned = jnp.concatenate([scaled, jnp.zeros((112, 512), F32)], axis=0).T
    read_rows = []
    for n in range(16):
        column = turned[:, n : n + 1]
        acc = jnp.zeros((8, 512), F32)
        for j in range(64):
            acc = acc + column[8 * j : 8 * j + 8] * mem[n, 0, 8 * j : 8 * j + 8, :]
        read_rows.append(jnp.sum(acc, axis=0, keepdims=True))
    read = score * value + jnp.concatenate(read_rows, axis=0)
    centered = read - jnp.mean(read, axis=1, keepdims=True)
    gated = centered * rms_scale(centered) * hg[...] * jax.nn.sigmoid(outgate)
    out[...] = gated.astype(BF)


def read(own, came, gates, head_gain, memory):
    vmem = pl.BlockSpec(memory_space=pltpu.VMEM)
    return pl.pallas_call(
        read_kernel,
        in_specs=[vmem] * 7,
        out_specs=vmem,
        out_shape=pltpu.VMEM((16, 512), BF),
        compiler_params=kernel_room(8),
        name="read",
    )(*on_chip(own, *came), gates, head_gain[None], memory)


def down_kernel(at, g, d0, d1, d2, d3, e0, e1, e2, e3, part, send, gains, full):
    ep = at[1]
    z, y, c = ep // (Y * C), (ep // C) & 3, ep & 1
    lane = lax.broadcasted_iota(jnp.int32, (16, 128), 1)
    row = lax.broadcasted_iota(jnp.int32, (16, 128), 0)
    eye = jnp.where(lane == row, 1.0, 0.0).astype(BF)
    a = jnp.concatenate(
        [
            jnp.concatenate([g[...], jnp.zeros((16, 128), BF)], axis=1),
            jnp.concatenate([jnp.zeros((16, 512), BF), eye], axis=1),
        ],
        axis=0,
    )
    low = lax.broadcasted_iota(jnp.int32, (32, 128), 1) < 64
    turn = (((1,), (1,)), ((), ()))
    for s, (d, e) in enumerate(zip((d0, d1, d2, d3), (e0, e1, e2, e3))):
        mine = lax.dot_general(a, d[...], turn, preferred_element_type=F32)
        other = lax.dot_general(a, e[...], turn, preferred_element_type=F32)
        for t in range(Y):
            j = t // 2 * 128
            m, o = mine[:, j : j + 128], other[:, j : j + 128]
            first = jnp.where(c == 0, m, o)
            second = jnp.where(c == 0, o, m)
            if t % 2 == 0:
                block = jnp.where(low, first, pltpu.roll(second, 64, 1))
            else:
                block = jnp.where(low, pltpu.roll(first, 64, 1), second)
            off = pl.multiple_of(((z + (Z - s)) & 3) * 512 + ((y + (Y - t)) & 3) * 128, 128)
            full[:, pl.ds(off, 128)] = block
    part[...] = full[0:16]
    send[...] = full[0:16].astype(BF)
    mixed_gain = full[16:17] + full[17:18] + full[18:19]
    expert_gain = full[19:20] + full[20:21] + full[21:22]
    gains[...] = jnp.concatenate(
        [mixed_gain, expert_gain, jnp.zeros((6, mixed_gain.shape[1]), F32)], axis=0
    )


def down_project(at, gated, own, partner):
    vmem = pl.BlockSpec(memory_space=pltpu.VMEM)
    return pl.pallas_call(
        down_kernel,
        in_specs=[pl.BlockSpec(memory_space=pltpu.SMEM)] + [vmem] * 9,
        out_specs=[vmem] * 3,
        out_shape=[
            pltpu.VMEM((16, 2048), F32),
            pltpu.VMEM((16, 2048), BF),
            pltpu.VMEM((8, 2048), F32),
        ],
        scratch_shapes=[pltpu.VMEM((32, 2048), F32)],
        compiler_params=kernel_room(8),
        name="down_project",
    )(at, gated, *on_chip(*own, *partner))


def layer(
    tokens,
    mixer_gain,
    query_weight,
    key_weight,
    value_weight,
    outgate_weight,
    igate_weight,
    fgate_weight,
    memory,
    stabilizer,
    head_gain,
    down_weight,
    mixed_gain,
    expert_gain,
    routes,
    route_weights,
    gate_proj,
    up_proj,
    expert_down,
    output_gain,
):
    ep_count = lax.axis_size("ep")
    tp_index = lax.axis_index("tp")
    at = jnp.stack([tp_index, lax.axis_index("ep")]).astype(jnp.int32)
    _, width = tokens.shape
    tp_width = output_gain.shape[0]

    tokens_float = tokens.astype(F32)
    w0 = join((query_weight, key_weight, value_weight, outgate_weight))
    by_z = [along_z(w0, s) for s in (2, 1, 3)]
    by_z = [w0, by_z[1], by_z[0], by_z[2]]
    packed, gates, send_from, take_with = prepare(
        at, tokens, mixer_gain, igate_weight, fgate_weight, down_weight, mixed_gain,
        expert_gain, stabilizer, routes, route_weights,
    )
    by_y = [along_y(packed, s) for s in (2, 1, 3)]
    by_y = [packed, by_y[1], by_y[0], by_y[2]]
    partner = [other_core(w) for w in by_z]
    down_y = jnp.concatenate([p[:, :640] for p in by_y], axis=0)
    down_z = [along_z(down_y, s) for s in (2, 1, 3)]
    down_z = [down_y, down_z[1], down_z[0], down_z[2]]
    own, t1, t2, t3 = project(at, by_y, by_z, partner)
    came = [along_y(t, -s) for s, t in ((2, t2), (1, t1), (3, t3))]
    down_partner = [other_core(d) for d in down_z]
    held = fetch(memory)
    gated = read(own, came, gates, head_gain, held)
    part, send, gains = down_project(at, gated, down_z, down_partner)
    mixed = part
    for s in (1, 2, 3):
        mixed = mixed + along_tp(send, s).astype(F32)

    residual_float = tokens_float + mixed * rms_scale(mixed) * gains[0]
    residual = lax.dynamic_slice_in_dim(residual_float.astype(BF), tp_index * tp_width, tp_width, 1)
    expert_in = (residual_float * rms_scale(residual_float) * gains[1]).astype(BF)
    outgoing = lax.dot_general(
        send_from.astype(BF), expert_in, (((0,), (0,)), ((), ())), preferred_element_type=F32
    ).astype(BF)
    arrived = lax.all_to_all(
        outgoing.reshape(ep_count, CAP, width), "ep", 0, 0, tiled=True
    ).reshape(ep_count * CAP, width)

    gate_pre = jnp.minimum(jnp.dot(arrived, gate_proj[0], preferred_element_type=F32), CLAMP_LIMIT)
    up_pre = jnp.clip(
        jnp.dot(arrived, up_proj[0], preferred_element_type=F32), -CLAMP_LIMIT, CLAMP_LIMIT
    )
    activation = ((up_pre + 1.0) * gate_pre * jax.nn.sigmoid(SIGMOID_SCALE * gate_pre)).astype(BF)
    partial_value = jnp.dot(activation, expert_down[0], preferred_element_type=F32)
    returned = lax.all_to_all(
        partial_value.astype(BF).reshape(ep_count, CAP, width), "ep", 0, 0, tiled=True
    ).reshape(ep_count * CAP, width)

    partial = jnp.dot(
        take_with, returned.astype(F32), precision=lax.Precision.HIGHEST,
        preferred_element_type=F32,
    )
    partial_sent = partial.astype(BF)
    combined = partial
    for s in (1, 2, 3):
        combined = combined + along_tp(partial_sent, s).astype(F32)
    scale = rms_scale(combined)
    combined_mine = lax.dynamic_slice_in_dim(combined, tp_index * tp_width, tp_width, 1)
    final_rows = residual.astype(F32) + combined_mine * scale * output_gain
    return final_rows.astype(BF)


def solution(mesh):
    placed = (
        P("ep", None),
        P(),
        P("ep", "tp"),
        P("ep", "tp"),
        P("ep", "tp"),
        P("ep", "tp"),
        P("tp", None),
        P("tp", None),
        P("ep", "tp", None, None),
        P("ep", "tp"),
        P("tp"),
        P(None, "ep"),
        P("ep"),
        P("ep"),
        P(),
        P(),
        P("ep", None, "tp"),
        P("ep", None, "tp"),
        P("ep", "tp", None),
        P("tp"),
    )
    return jax.shard_map(
        layer, mesh=mesh, in_specs=placed, out_specs=P("ep", "tp"), check_vma=False
    )
```

```python
import jax
import jax.numpy as jnp
from jax import lax
from jax.experimental import pallas as pl
from jax.experimental.pallas import tpu as pltpu
from jax.sharding import PartitionSpec as P


NORM_EPS = 1e-06
CLAMP_LIMIT = 7.0
SIGMOID_SCALE = 1.702
BF = jnp.bfloat16
F32 = jnp.float32
Z, Y, C, TP = 4, 4, 2, 4


def ep_at(z, y, c):
    return (z % Z) * (Y * C) + (y % Y) * C + c % C


def ep_moves(dz, dy, dc):
    return [
        (ep_at(z, y, c), ep_at(z + dz, y + dy, c + dc))
        for z in range(Z)
        for y in range(Y)
        for c in range(C)
    ]


def along_z(a, s):
    return lax.ppermute(a, "ep", ep_moves(s, 0, 0))


def along_y(a, s):
    return lax.ppermute(a, "ep", ep_moves(0, s, 0))


def other_core(a):
    return lax.ppermute(a, "ep", ep_moves(0, 0, 1))


def along_tp(a, s):
    return lax.ppermute(a, "tp", [(i, (i + s) % TP) for i in range(TP)])


def on_chip(*arrays):
    return [pltpu.with_memory_space_constraint(a, pltpu.VMEM) for a in arrays]


def kernel_room(mebibytes):
    return pltpu.CompilerParams(vmem_limit_bytes=mebibytes << 20)


def rms_scale(values):
    return lax.rsqrt(jnp.mean(values * values, axis=-1, keepdims=True) + NORM_EPS)


def join_kernel(q, k, v, o, w0, sems):
    loads = [
        pltpu.make_async_copy(r, w0.at[:, pl.ds(i * 512, 512)], sems.at[i])
        for i, r in enumerate((q, k, v, o))
    ]
    for load in loads:
        load.start()
    for load in loads:
        load.wait()


def join(weights):
    return pl.pallas_call(
        join_kernel,
        in_specs=[pl.BlockSpec(memory_space=pl.ANY)] * 4,
        out_specs=pl.BlockSpec(memory_space=pltpu.VMEM),
        out_shape=pltpu.VMEM((64, 2048), BF),
        scratch_shapes=[pltpu.SemaphoreType.DMA((4,))],
        name="join",
    )(*weights)


def normed_of(x, gain):
    xf = x[...].astype(F32)
    return (xf * rms_scale(xf) * gain[...]).astype(BF)


def split_in_three(whole):
    high = whole.astype(BF).astype(F32)
    rest = whole - high
    mid = rest.astype(BF).astype(F32)
    return high, mid, rest - mid


TURNED = (((1,), (1,)), ((), ()))


def prepare_kernel(x, gain, dw, mg, eg, out0, out1, out2, out3, normed, down, sem):
    y = (lax.axis_index("ep") // C) & 3
    col = pl.multiple_of(lax.axis_index("tp") * 512, 128)
    load = pltpu.make_async_copy(dw.at[:, pl.ds(col, 512)], down, sem)
    load.start()
    normed[...] = normed_of(x, gain)
    row = lax.broadcasted_iota(jnp.int32, (8, 64), 0)
    extra = jnp.zeros((8, 64), F32)
    for i, g in enumerate((mg, eg)):
        for j, piece in enumerate(split_in_three(g[...])):
            extra = jnp.where(row == 3 * i + j, piece, extra)
    extra = jnp.concatenate([extra, jnp.zeros((8, 576), F32)], axis=1).astype(BF)
    load.wait()
    for s, out in enumerate((out0, out1, out2, out3)):
        out[0:64, 0:512] = down[...]
        out[64:72] = extra
        target = (y + s) & 3
        for i in range(Z):
            off = pl.multiple_of(512 * i + target * 128, 128)
            out[16 * i : 16 * i + 16, 512:640] = normed[:, pl.ds(off, 128)]


def prepare(tokens, mixer_gain, down_weight, mg, eg):
    vmem = pl.BlockSpec(memory_space=pltpu.VMEM)
    return pl.pallas_call(
        prepare_kernel,
        in_specs=[vmem, vmem, pl.BlockSpec(memory_space=pl.ANY), vmem, vmem],
        out_specs=[vmem] * 4,
        out_shape=[pltpu.VMEM((72, 640), BF)] * 4,
        scratch_shapes=[
            pltpu.VMEM((16, 2048), BF),
            pltpu.VMEM((64, 512), BF),
            pltpu.SemaphoreType.DMA,
        ],
        name="prepare",
    )(tokens, mixer_gain[None], down_weight.T, mg[None], eg[None])


def route_kernel(x, gain, ig, fg, stab, routes, weights, gates, send, take):
    nf = normed_of(x, gain).astype(F32)
    log_input = jnp.sum(nf * ig[...].astype(F32), axis=1, keepdims=True)
    pre = jnp.sum(nf * fg[...].astype(F32), axis=1, keepdims=True)
    log_forget = jnp.minimum(pre, 0.0) - jnp.log1p(jnp.exp(-jnp.abs(pre)))
    small = lax.broadcasted_iota(jnp.int32, (16, 16), 0)
    across = lax.broadcasted_iota(jnp.int32, (16, 16), 1)
    stab_column = jnp.sum(jnp.where(small == across, stab[...], 0.0), axis=1, keepdims=True)
    first = lax.broadcasted_iota(jnp.int32, (16, 128), 1)
    gates[...] = jnp.where(first == 0, log_input, log_forget + stab_column)
    pick = jnp.where(
        lax.broadcasted_iota(jnp.int32, (16, 512), 1)
        == lax.broadcasted_iota(jnp.int32, (16, 512), 0) + lax.axis_index("ep") * 16,
        1.0,
        0.0,
    )
    chosen = lax.dot_general(
        pick, routes[...].astype(F32), TURNED, precision=lax.Precision.HIGHEST,
        preferred_element_type=F32,
    )
    weight = lax.dot_general(
        pick, weights[...], TURNED, precision=lax.Precision.HIGHEST, preferred_element_type=F32
    )
    lane = lax.broadcasted_iota(jnp.int32, (16, 256), 1)
    expert_of = (lane >> 3).astype(F32)
    named = jnp.zeros((16, 256), F32)
    weight_of = jnp.zeros((16, 256), F32)
    for k in range(4):
        hit = chosen[:, k : k + 1] == expert_of
        named = jnp.where(hit, 1.0, named)
        weight_of = jnp.where(hit, weight[:, k : k + 1], weight_of)
    before = jnp.dot(
        jnp.where(small > across, 1.0, 0.0).astype(BF), named.astype(BF),
        preferred_element_type=F32,
    )
    placed = (named > 0.5) & (before == (lane & 3).astype(F32))
    for h in range(2):
        half = placed & (((lane >> 2) & 1) == h)
        send[16 * h : 16 * h + 16] = jnp.where(half, 1.0, 0.0).astype(BF)
        taken = jnp.where(half, weight_of, 0.0)
        for j, piece in enumerate(split_in_three(taken)):
            at = 48 * h + 16 * j
            take[at : at + 16] = piece.astype(BF)


def route(tokens, mixer_gain, ig, fg, stabilizer, routes, weights):
    vmem = pl.BlockSpec(memory_space=pltpu.VMEM)
    return pl.pallas_call(
        route_kernel,
        in_specs=[vmem] * 7,
        out_specs=[vmem] * 3,
        out_shape=[
            pltpu.VMEM((16, 128), F32),
            pltpu.VMEM((32, 256), BF),
            pltpu.VMEM((96, 256), BF),
        ],
        name="route",
    )(tokens, mixer_gain[None], ig, fg, stabilizer.T, routes.T, weights.T)


def stack_kernel(a0, a1, a2, a3, out):
    for i, a in enumerate((a0, a1, a2, a3)):
        out[64 * i : 64 * i + 64] = a[0:64, 0:512]
        out[256 + 8 * i : 264 + 8 * i] = a[64:72, 0:512]


def stack_down(pieces):
    vmem = pl.BlockSpec(memory_space=pltpu.VMEM)
    return pl.pallas_call(
        stack_kernel,
        in_specs=[vmem] * 4,
        out_specs=vmem,
        out_shape=pltpu.VMEM((288, 512), BF),
        compiler_params=kernel_room(4),
        name="stack_down",
    )(*on_chip(*pieces))


def project_kernel(
    n0, n1, n2, n3, w0, w1, w2, w3, p0, p1, p2, p3, own, t1, t2, t3
):
    ep = lax.axis_index("ep")
    z, c = ep // (Y * C), ep & 1
    rows = []
    for n in (n0, n1, n2, n3):
        chunks = []
        for s in range(Z):
            off = pl.multiple_of(((z + (Z - s)) & 3) * 16, 16)
            part = n[pl.ds(off, 16), 512:640].astype(F32)
            chunks.append(jnp.where(c == 0, part, pltpu.roll(part, 64, 1)).astype(BF))
        rows.append(jnp.concatenate(chunks, axis=1))
    x = jnp.concatenate(rows, axis=0)
    pieces = [r for pair in zip((w0, w1, w2, w3), (p0, p1, p2, p3)) for r in pair]
    for i in range(4):
        at_i = slice(512 * i, 512 * (i + 1))
        w = jnp.concatenate([r[:, at_i] for r in pieces], axis=0)
        acc = jnp.dot(x, w, preferred_element_type=F32)
        own[:, at_i] = acc[0:16]
        for k, t in ((16, t1), (32, t2), (48, t3)):
            part = acc[k : k + 16]
            high = part.astype(BF)
            t[:, at_i] = high
            if i < 2:
                low = (part - high.astype(F32)).astype(BF)
                t[:, 2048 + 512 * i : 2048 + 512 * (i + 1)] = low


def project(packed_by_shift, weights, partner):
    rows, width = 16, weights[0].shape[1]
    vmem = pl.BlockSpec(memory_space=pltpu.VMEM)
    return pl.pallas_call(
        project_kernel,
        in_specs=[vmem] * 12,
        out_specs=[vmem] * 4,
        out_shape=[pltpu.VMEM((rows, width), F32)]
        + [pltpu.VMEM((rows, width + width // 2), BF)] * 3,
        compiler_params=kernel_room(8),
        name="project",
    )(*on_chip(*packed_by_shift, *weights, *partner))


def fetch_kernel(memory, out, sems):
    loads = [
        pltpu.make_async_copy(memory.at[n], out.at[n], sems.at[n]) for n in range(out.shape[0])
    ]
    for load in loads:
        load.start()
    for load in loads:
        load.wait()


def fetch(memory):
    return pl.pallas_call(
        fetch_kernel,
        in_specs=[pl.BlockSpec(memory_space=pltpu.HBM)],
        out_specs=pl.BlockSpec(memory_space=pltpu.VMEM),
        out_shape=pltpu.VMEM(memory.shape, F32),
        scratch_shapes=[pltpu.SemaphoreType.DMA((memory.shape[0],))],
        compiler_params=kernel_room(4),
        name="fetch",
    )(pltpu.with_memory_space_constraint(memory, pltpu.HBM))


def read_kernel(own, r1, r2, r3, gates, hg, mem, out):
    parts = []
    for i in range(4):
        at_i = slice(512 * i, 512 * (i + 1))
        total = own[:, at_i]
        for r in (r1, r2, r3):
            came = r[:, at_i].astype(F32)
            if i < 2:
                came = came + r[:, 2048 + 512 * i : 2048 + 512 * (i + 1)].astype(F32)
            total = total + came
        parts.append(total.astype(BF).astype(F32))
    query, key, value, outgate = parts
    query = query * 512 ** (-0.5)
    log_input, carry = gates[:, 0:1], gates[:, 1:2]
    peak = jnp.maximum(carry, log_input)
    within = jnp.exp(log_input - peak)
    carried = jnp.exp(carry - peak)
    score = jnp.sum(query * key, axis=1, keepdims=True) * within
    scaled = query * carried
    turned = jnp.concatenate([scaled, jnp.zeros((112, 512), F32)], axis=0).T
    read_rows = []
    for n in range(16):
        column = turned[:, n : n + 1]
        acc = jnp.zeros((8, 512), F32)
        for j in range(64):
            acc = acc + column[8 * j : 8 * j + 8] * mem[n, 0, 8 * j : 8 * j + 8, :]
        read_rows.append(jnp.sum(acc, axis=0, keepdims=True))
    read = score * value + jnp.concatenate(read_rows, axis=0)
    centered = read - jnp.mean(read, axis=1, keepdims=True)
    gated = centered * rms_scale(centered) * hg[...] * jax.nn.sigmoid(outgate)
    out[...] = gated.astype(BF)


def read(own, came, gates, head_gain, memory):
    vmem = pl.BlockSpec(memory_space=pltpu.VMEM)
    return pl.pallas_call(
        read_kernel,
        in_specs=[vmem] * 7,
        out_specs=vmem,
        out_shape=pltpu.VMEM((16, 512), BF),
        compiler_params=kernel_room(8),
        name="read",
    )(*on_chip(own, *came), gates, head_gain[None], memory)


def paired(mine, other, c, odd):
    first = jnp.where(c == 0, mine, other)
    second = jnp.where(c == 0, other, mine)
    low = lax.broadcasted_iota(jnp.int32, mine.shape, 1) < 64
    if odd:
        return jnp.where(low, pltpu.roll(first, 64, 1), second)
    return jnp.where(low, first, pltpu.roll(second, 64, 1))


def down_kernel(g, d0, d1, d2, d3, e0, e1, e2, e3, part, send, gains, factors):
    ep = lax.axis_index("ep")
    z, y, c = ep // (Y * C), (ep // C) & 3, ep & 1
    gated = g[...]
    for s, (d, e) in enumerate(zip((d0, d1, d2, d3), (e0, e1, e2, e3))):
        mine = lax.dot_general(gated, d[0:256], TURNED, preferred_element_type=F32)
        other = lax.dot_general(gated, e[0:256], TURNED, preferred_element_type=F32)
        my_gains = d[256:288, 0:128].astype(F32)
        other_gains = e[256:288, 0:128].astype(F32)
        for t in range(Y):
            at = slice(t // 2 * 128, t // 2 * 128 + 128)
            block = paired(mine[:, at], other[:, at], c, t % 2 == 1)
            off = pl.multiple_of(((z + (Z - s)) & 3) * 512 + ((y + (Y - t)) & 3) * 128, 128)
            part[:, pl.ds(off, 128)] = block
            send[:, pl.ds(off, 128)] = block.astype(BF)
            at = slice(8 * t, 8 * t + 8)
            factors[:, pl.ds(off, 128)] = paired(my_gains[at], other_gains[at], c, False)
    gains[0:1] = factors[0:1] + factors[1:2] + factors[2:3]
    gains[1:2] = factors[3:4] + factors[4:5] + factors[5:6]


def down_project(gated, own, partner):
    vmem = pl.BlockSpec(memory_space=pltpu.VMEM)
    return pl.pallas_call(
        down_kernel,
        in_specs=[vmem] * 9,
        out_specs=[vmem] * 3,
        out_shape=[
            pltpu.VMEM((16, 2048), F32),
            pltpu.VMEM((16, 2048), BF),
            pltpu.VMEM((8, 2048), F32),
        ],
        scratch_shapes=[pltpu.VMEM((8, 2048), F32)],
        compiler_params=kernel_room(8),
        name="down_project",
    )(gated, *on_chip(*own, *partner))


def fetch_experts_kernel(g, u, d, gate, up, down, sems):
    loads = [
        pltpu.make_async_copy(r.at[0], o, sems.at[i])
        for i, (r, o) in enumerate(((g, gate), (u, up), (d, down)))
    ]
    for load in loads:
        load.start()
    for load in loads:
        load.wait()


def fetch_experts(*arrays):
    return pl.pallas_call(
        fetch_experts_kernel,
        in_specs=[pl.BlockSpec(memory_space=pltpu.HBM)] * 3,
        out_specs=[pl.BlockSpec(memory_space=pltpu.VMEM)] * 3,
        out_shape=[pltpu.VMEM(a.shape[1:], BF) for a in arrays],
        scratch_shapes=[pltpu.SemaphoreType.DMA((3,))],
        compiler_params=kernel_room(4),
        name="fetch_experts",
    )(*[pltpu.with_memory_space_constraint(a, pltpu.HBM) for a in arrays])


def dispatch_kernel(x, part, r1, r2, r3, gains, send, residual, outgoing):
    mixed = part[...] + r1[...].astype(F32) + r2[...].astype(F32) + r3[...].astype(F32)
    total = x[...].astype(F32) + mixed * rms_scale(mixed) * gains[0:1]
    residual[...] = total.astype(BF)
    expert_in = (total * rms_scale(total) * gains[1:2]).astype(BF)
    halves = jnp.concatenate([expert_in[:, 0:1024], expert_in[:, 1024:2048]], axis=0)
    outgoing[...] = lax.dot_general(
        send[...], halves, (((0,), (0,)), ((), ())), preferred_element_type=F32
    ).astype(BF)


def dispatch(tokens, part, came, gains, send_from):
    vmem = pl.BlockSpec(memory_space=pltpu.VMEM)
    return pl.pallas_call(
        dispatch_kernel,
        in_specs=[vmem] * 7,
        out_specs=[vmem] * 2,
        out_shape=[pltpu.VMEM((16, 2048), BF), pltpu.VMEM((256, 1024), BF)],
        compiler_params=kernel_room(8),
        name="dispatch",
    )(tokens, part, *on_chip(*came), gains, send_from)


def experts_kernel(arrived, gate_w, up_w, down_w, out):
    row = lax.broadcasted_iota(jnp.int32, (128, 256), 0)
    lane = lax.broadcasted_iota(jnp.int32, (128, 256), 1)
    place = ((row >> 2) << 3) + (row & 3)
    rows = jnp.concatenate(
        [
            jnp.dot(
                jnp.where(lane == place + 4 * h, 1.0, 0.0).astype(BF), arrived[...],
                preferred_element_type=F32,
            ).astype(BF)
            for h in range(2)
        ],
        axis=1,
    )
    gate = jnp.minimum(jnp.dot(rows, gate_w[...], preferred_element_type=F32), CLAMP_LIMIT)
    up = jnp.clip(
        jnp.dot(rows, up_w[...], preferred_element_type=F32), -CLAMP_LIMIT, CLAMP_LIMIT
    )
    activation = ((up + 1.0) * gate * jax.nn.sigmoid(SIGMOID_SCALE * gate)).astype(BF)
    value = jnp.dot(activation, down_w[...], preferred_element_type=F32).astype(BF)
    both = jnp.concatenate([value[:, 0:1024], value[:, 1024:2048]], axis=0)
    goes = lax.broadcasted_iota(jnp.int32, (256, 256), 0)
    source = lax.broadcasted_iota(jnp.int32, (256, 256), 1)
    wanted = ((goes >> 2) & 1) * 128 + ((goes >> 3) << 2) + (goes & 3)
    out[...] = jnp.dot(
        jnp.where(source == wanted, 1.0, 0.0).astype(BF), both, preferred_element_type=F32
    ).astype(BF)


def run_experts(arrived, weights):
    vmem = pl.BlockSpec(memory_space=pltpu.VMEM)
    return pl.pallas_call(
        experts_kernel,
        in_specs=[vmem] * 4,
        out_specs=vmem,
        out_shape=pltpu.VMEM(arrived.shape, BF),
        compiler_params=kernel_room(16),
        name="experts",
    )(*on_chip(arrived), *weights)


def combine_kernel(take, returned, part, send):
    sums = jnp.dot(take[...], returned[...], preferred_element_type=F32)
    for h in range(2):
        at = 48 * h
        half = sums[at : at + 16] + sums[at + 16 : at + 32] + sums[at + 32 : at + 48]
        part[:, 1024 * h : 1024 * (h + 1)] = half
        send[:, 1024 * h : 1024 * (h + 1)] = half.astype(BF)


def combine(take_with, returned):
    vmem = pl.BlockSpec(memory_space=pltpu.VMEM)
    return pl.pallas_call(
        combine_kernel,
        in_specs=[vmem] * 2,
        out_specs=[vmem] * 2,
        out_shape=[pltpu.VMEM((16, 2048), F32), pltpu.VMEM((16, 2048), BF)],
        compiler_params=kernel_room(8),
        name="combine",
    )(take_with, *on_chip(returned))


def finish_kernel(part, r1, r2, r3, residual, gain, out, total):
    combined = part[...] + r1[...].astype(F32) + r2[...].astype(F32) + r3[...].astype(F32)
    scale = rms_scale(combined)
    total[...] = combined
    col = pl.multiple_of(lax.axis_index("tp") * 512, 128)
    mine = total[:, pl.ds(col, 512)]
    out[...] = (residual[:, pl.ds(col, 512)].astype(F32) + mine * scale * gain[...]).astype(BF)


def finish(part, came, residual, output_gain):
    vmem = pl.BlockSpec(memory_space=pltpu.VMEM)
    return pl.pallas_call(
        finish_kernel,
        in_specs=[vmem] * 6,
        out_specs=vmem,
        out_shape=jax.ShapeDtypeStruct((16, 512), BF),
        scratch_shapes=[pltpu.VMEM((16, 2048), F32)],
        compiler_params=kernel_room(8),
        name="finish",
    )(part, *on_chip(*came), residual, output_gain[None])


def layer(
    tokens,
    mixer_gain,
    query_weight,
    key_weight,
    value_weight,
    outgate_weight,
    igate_weight,
    fgate_weight,
    memory,
    stabilizer,
    head_gain,
    down_weight,
    mixed_gain,
    expert_gain,
    routes,
    route_weights,
    gate_proj,
    up_proj,
    expert_down,
    output_gain,
):
    ep_count = lax.axis_size("ep")
    packed = prepare(tokens, mixer_gain, down_weight, mixed_gain, expert_gain)
    by_y = [along_y(packed[s], s) for s in (2, 1, 3)]
    by_y = [packed[0], by_y[1], by_y[0], by_y[2]]
    w0 = join((query_weight, key_weight, value_weight, outgate_weight))
    by_z = [along_z(w0, s) for s in (2, 1, 3)]
    by_z = [w0, by_z[1], by_z[0], by_z[2]]
    gates, send_from, take_with = route(
        tokens, mixer_gain, igate_weight, fgate_weight, stabilizer, routes, route_weights
    )
    down_y = stack_down(by_y)
    down_z = [along_z(down_y, s) for s in (2, 1, 3)]
    down_z = [down_y, down_z[1], down_z[0], down_z[2]]
    held = fetch(memory)
    partner = [other_core(w) for w in by_z]
    own, t1, t2, t3 = project(by_y, by_z, partner)
    came = [along_y(t, -s) for s, t in ((2, t2), (1, t1), (3, t3))]
    down_partner = [other_core(d) for d in down_z]
    gated = read(own, came, gates, head_gain, held)
    part, send, gains = down_project(gated, down_z, down_partner)
    mixed = [along_tp(send, s) for s in (2, 1, 3)]
    weights = fetch_experts(gate_proj, up_proj, expert_down)
    residual, outgoing = dispatch(tokens, part, mixed, gains, send_from)
    arrived = lax.all_to_all(
        outgoing.reshape(ep_count, 8, 1024), "ep", 0, 0, tiled=True
    ).reshape(256, 1024)
    value = run_experts(arrived, weights)
    returned = lax.all_to_all(
        value.reshape(ep_count, 8, 1024), "ep", 0, 0, tiled=True
    ).reshape(256, 1024)
    own_sum, sent = combine(take_with, returned)
    others = [along_tp(sent, s) for s in (2, 1, 3)]
    return finish(own_sum, others, residual, output_gain)


def solution(mesh):
    placed = (
        P("ep", None),
        P(),
        P("ep", "tp"),
        P("ep", "tp"),
        P("ep", "tp"),
        P("ep", "tp"),
        P("tp", None),
        P("tp", None),
        P("ep", "tp", None, None),
        P("ep", "tp"),
        P("tp"),
        P(None, "ep"),
        P("ep"),
        P("ep"),
        P(),
        P(),
        P("ep", None, "tp"),
        P("ep", None, "tp"),
        P("ep", "tp", None),
        P("tp"),
    )
    return jax.shard_map(
        layer, mesh=mesh, in_specs=placed, out_specs=P("ep", "tp"), check_vma=False
    )
```

```python
import jax
import jax.numpy as jnp
from jax import lax
from jax.experimental import pallas as pl
from jax.experimental.pallas import tpu as pltpu
from jax.sharding import PartitionSpec as P


NORM_EPS = 1e-06
CLAMP_LIMIT = 7.0
SIGMOID_SCALE = 1.702
BF = jnp.bfloat16
F32 = jnp.float32
Z, Y, C, TP = 4, 4, 2, 4
EARLY, HELD = 4, 12


def ep_at(z, y, c):
    return (z % Z) * (Y * C) + (y % Y) * C + c % C


def ep_moves(dz, dy, dc):
    return [
        (ep_at(z, y, c), ep_at(z + dz, y + dy, c + dc))
        for z in range(Z)
        for y in range(Y)
        for c in range(C)
    ]


def along_z(a, s):
    return lax.ppermute(a, "ep", ep_moves(s, 0, 0))


def along_y(a, s):
    return lax.ppermute(a, "ep", ep_moves(0, s, 0))


def spread(send, order):
    came = {}
    for s in order:
        came[s] = send(s)
    return [came[s] for s in (1, 2, 3)]


NEAR_FIRST, FAR_FIRST = (1, 3, 2), (2, 1, 3)


def other_core(a):
    return lax.ppermute(a, "ep", ep_moves(0, 0, 1))


def along_tp(a, s):
    return lax.ppermute(a, "tp", [(i, (i + s) % TP) for i in range(TP)])


def on_chip(*arrays):
    return [pltpu.with_memory_space_constraint(a, pltpu.VMEM) for a in arrays]


def kernel_room(mebibytes):
    return pltpu.CompilerParams(vmem_limit_bytes=mebibytes << 20)


def rms_scale(values):
    return lax.rsqrt(jnp.mean(values * values, axis=-1, keepdims=True) + NORM_EPS)


def join_kernel(q, k, v, o, w0, sems):
    loads = [
        pltpu.make_async_copy(r, w0.at[:, pl.ds(i * 512, 512)], sems.at[i])
        for i, r in enumerate((q, k, v, o))
    ]
    for load in loads:
        load.start()
    for load in loads:
        load.wait()


def join(weights):
    return pl.pallas_call(
        join_kernel,
        in_specs=[pl.BlockSpec(memory_space=pl.ANY)] * 4,
        out_specs=pl.BlockSpec(memory_space=pltpu.VMEM),
        out_shape=pltpu.VMEM((64, 2048), BF),
        scratch_shapes=[pltpu.SemaphoreType.DMA((4,))],
        name="join",
    )(*weights)


def normed_of(x, gain):
    xf = x[...].astype(F32)
    return (xf * rms_scale(xf) * gain[...]).astype(BF)


def split_in_three(whole):
    high = whole.astype(BF).astype(F32)
    rest = whole - high
    mid = rest.astype(BF).astype(F32)
    return high, mid, rest - mid


TURNED = (((1,), (1,)), ((), ()))


def prepare_kernel(
    x_in, gain_in, dw, mg_in, eg_in, ig_in, fg_in, stab_in, memory,
    out0, out1, out2, out3, gates, early,
    x, gain, mg, eg, ig, fg, stab, normed, down, sems, row_sems,
):
    y = (lax.axis_index("ep") // C) & 3
    col = pl.multiple_of(lax.axis_index("tp") * 512, 128)
    pairs = (
        (x_in, x), (gain_in, gain), (mg_in, mg), (eg_in, eg), (ig_in, ig), (fg_in, fg),
        (stab_in, stab), (dw.at[:, pl.ds(col, 512)], down),
    )
    loads = [pltpu.make_async_copy(a, b, sems.at[i]) for i, (a, b) in enumerate(pairs)]
    rows = [
        pltpu.make_async_copy(memory.at[i], early.at[i], row_sems.at[i]) for i in range(EARLY)
    ]
    for load in loads + rows:
        load.start()
    for load in loads:
        load.wait()
    normed[...] = normed_of(x, gain)
    nf = normed[...].astype(F32)
    log_input = jnp.sum(nf * ig[...].astype(F32), axis=1, keepdims=True)
    pre = jnp.sum(nf * fg[...].astype(F32), axis=1, keepdims=True)
    log_forget = jnp.minimum(pre, 0.0) - jnp.log1p(jnp.exp(-jnp.abs(pre)))
    small = lax.broadcasted_iota(jnp.int32, (16, 16), 0)
    across = lax.broadcasted_iota(jnp.int32, (16, 16), 1)
    stab_column = jnp.sum(jnp.where(small == across, stab[...], 0.0), axis=1, keepdims=True)
    first = lax.broadcasted_iota(jnp.int32, (16, 128), 1)
    gates[...] = jnp.where(first == 0, log_input, log_forget + stab_column)
    row = lax.broadcasted_iota(jnp.int32, (8, 64), 0)
    extra = jnp.zeros((8, 64), F32)
    for i, g in enumerate((mg, eg)):
        for j, piece in enumerate(split_in_three(g[...])):
            extra = jnp.where(row == 3 * i + j, piece, extra)
    extra = jnp.concatenate([extra, jnp.zeros((8, 576), F32)], axis=1).astype(BF)
    for s, out in enumerate((out0, out1, out2, out3)):
        out[0:64, 0:512] = down[...]
        out[64:72] = extra
        target = (y + s) & 3
        for i in range(Z):
            off = pl.multiple_of(512 * i + target * 128, 128)
            out[16 * i : 16 * i + 16, 512:640] = normed[:, pl.ds(off, 128)]
    for load in rows:
        load.wait()


def prepare(tokens, mixer_gain, down_weight, mg, eg, ig, fg, stabilizer, memory):
    vmem = pl.BlockSpec(memory_space=pltpu.VMEM)
    ins = [tokens, mixer_gain[None], down_weight.T, mg[None], eg[None], ig, fg, stabilizer.T]
    ins = [pltpu.with_memory_space_constraint(a, pltpu.HBM) for a in ins + [memory]]
    return pl.pallas_call(
        prepare_kernel,
        in_specs=[pl.BlockSpec(memory_space=pltpu.HBM)] * 9,
        out_specs=[vmem] * 6,
        out_shape=[pltpu.VMEM((72, 640), BF)] * 4
        + [pltpu.VMEM((16, 128), F32), pltpu.VMEM((EARLY, *memory.shape[1:]), F32)],
        scratch_shapes=[pltpu.VMEM(ins[i].shape, ins[i].dtype) for i in (0, 1, 3, 4, 5, 6, 7)]
        + [
            pltpu.VMEM((16, 2048), BF),
            pltpu.VMEM((64, 512), BF),
            pltpu.SemaphoreType.DMA((8,)),
            pltpu.SemaphoreType.DMA((EARLY,)),
        ],
        compiler_params=kernel_room(4),
        name="prepare",
    )(*ins)


def route_kernel(routes, weights, send, take):
    small = lax.broadcasted_iota(jnp.int32, (16, 16), 0)
    across = lax.broadcasted_iota(jnp.int32, (16, 16), 1)
    pick = jnp.where(
        lax.broadcasted_iota(jnp.int32, (16, 512), 1)
        == lax.broadcasted_iota(jnp.int32, (16, 512), 0) + lax.axis_index("ep") * 16,
        1.0,
        0.0,
    )
    chosen = lax.dot_general(
        pick, routes[...].astype(F32), TURNED, precision=lax.Precision.HIGHEST,
        preferred_element_type=F32,
    )
    weight = lax.dot_general(
        pick, weights[...], TURNED, precision=lax.Precision.HIGHEST, preferred_element_type=F32
    )
    lane = lax.broadcasted_iota(jnp.int32, (16, 256), 1)
    expert_of = (lane >> 3).astype(F32)
    named = jnp.zeros((16, 256), F32)
    weight_of = jnp.zeros((16, 256), F32)
    for k in range(4):
        hit = chosen[:, k : k + 1] == expert_of
        named = jnp.where(hit, 1.0, named)
        weight_of = jnp.where(hit, weight[:, k : k + 1], weight_of)
    before = jnp.dot(
        jnp.where(small > across, 1.0, 0.0).astype(BF), named.astype(BF),
        preferred_element_type=F32,
    )
    placed = (named > 0.5) & (before == (lane & 3).astype(F32))
    for h in range(2):
        half = placed & (((lane >> 2) & 1) == h)
        send[16 * h : 16 * h + 16] = jnp.where(half, 1.0, 0.0).astype(BF)
        taken = jnp.where(half, weight_of, 0.0)
        for j, piece in enumerate(split_in_three(taken)):
            at = 48 * h + 16 * j
            take[at : at + 16] = piece.astype(BF)


def route(routes, weights):
    vmem = pl.BlockSpec(memory_space=pltpu.VMEM)
    return pl.pallas_call(
        route_kernel,
        in_specs=[vmem] * 2,
        out_specs=[vmem] * 2,
        out_shape=[
            pltpu.VMEM((32, 256), BF),
            pltpu.VMEM((96, 256), BF),
        ],
        compiler_params=kernel_room(4),
        name="route",
    )(routes.T, weights.T)


def stack_kernel(a0, a1, a2, a3, out):
    for i, a in enumerate((a0, a1, a2, a3)):
        out[64 * i : 64 * i + 64] = a[0:64, 0:512]
        out[256 + 8 * i : 264 + 8 * i] = a[64:72, 0:512]


def stack_down(pieces):
    vmem = pl.BlockSpec(memory_space=pltpu.VMEM)
    return pl.pallas_call(
        stack_kernel,
        in_specs=[vmem] * 4,
        out_specs=vmem,
        out_shape=pltpu.VMEM((288, 512), BF),
        compiler_params=kernel_room(4),
        name="stack_down",
    )(*on_chip(*pieces))


def project_kernel(
    n0, n1, n2, n3, w0, w1, w2, w3, p0, p1, p2, p3, own, t1, t2, t3
):
    ep = lax.axis_index("ep")
    z, c = ep // (Y * C), ep & 1
    rows = []
    for n in (n0, n1, n2, n3):
        chunks = []
        for s in range(Z):
            off = pl.multiple_of(((z + (Z - s)) & 3) * 16, 16)
            part = n[pl.ds(off, 16), 512:640].astype(F32)
            chunks.append(jnp.where(c == 0, part, pltpu.roll(part, 64, 1)).astype(BF))
        rows.append(jnp.concatenate(chunks, axis=1))
    x = jnp.concatenate(rows, axis=0)
    pieces = [r for pair in zip((w0, w1, w2, w3), (p0, p1, p2, p3)) for r in pair]
    for i in range(4):
        at_i = slice(512 * i, 512 * (i + 1))
        w = jnp.concatenate([r[:, at_i] for r in pieces], axis=0)
        acc = jnp.dot(x, w, preferred_element_type=F32)
        own[:, at_i] = acc[0:16]
        for k, t in ((16, t1), (32, t2), (48, t3)):
            part = acc[k : k + 16]
            high = part.astype(BF)
            t[:, at_i] = high
            if i < 2:
                low = (part - high.astype(F32)).astype(BF)
                t[:, 2048 + 512 * i : 2048 + 512 * (i + 1)] = low


def project(packed_by_shift, weights, partner):
    rows, width = 16, weights[0].shape[1]
    vmem = pl.BlockSpec(memory_space=pltpu.VMEM)
    return pl.pallas_call(
        project_kernel,
        in_specs=[vmem] * 12,
        out_specs=[vmem] * 4,
        out_shape=[pltpu.VMEM((rows, width), F32)]
        + [pltpu.VMEM((rows, width + width // 2), BF)] * 3,
        compiler_params=kernel_room(8),
        name="project",
    )(*on_chip(*packed_by_shift, *weights, *partner))


def fetch(memory, start, stop):
    def kernel(whole, out, sems):
        loads = [
            pltpu.make_async_copy(whole.at[start + i], out.at[i], sems.at[i])
            for i in range(stop - start)
        ]
        for load in loads:
            load.start()
        for load in loads:
            load.wait()

    return pl.pallas_call(
        kernel,
        in_specs=[pl.BlockSpec(memory_space=pltpu.HBM)],
        out_specs=pl.BlockSpec(memory_space=pltpu.VMEM),
        out_shape=pltpu.VMEM((stop - start, *memory.shape[1:]), F32),
        scratch_shapes=[pltpu.SemaphoreType.DMA((stop - start,))],
        compiler_params=kernel_room(4),
        name="fetch_rows",
    )(pltpu.with_memory_space_constraint(memory, pltpu.HBM))


def read_kernel(own, r1, r2, r3, gates, hg, early, held, memory, out, late, sems):
    loads = [
        pltpu.make_async_copy(memory.at[HELD + i], late.at[i], sems.at[i])
        for i in range(late.shape[0])
    ]
    for load in loads:
        load.start()
    parts = []
    for i in range(4):
        at_i = slice(512 * i, 512 * (i + 1))
        total = own[:, at_i]
        for r in (r1, r2, r3):
            came = r[:, at_i].astype(F32)
            if i < 2:
                came = came + r[:, 2048 + 512 * i : 2048 + 512 * (i + 1)].astype(F32)
            total = total + came
        parts.append(total.astype(BF).astype(F32))
    query, key, value, outgate = parts
    query = query * 512 ** (-0.5)
    log_input, carry = gates[:, 0:1], gates[:, 1:2]
    peak = jnp.maximum(carry, log_input)
    within = jnp.exp(log_input - peak)
    carried = jnp.exp(carry - peak)
    score = jnp.sum(query * key, axis=1, keepdims=True) * within
    scaled = query * carried
    turned = jnp.concatenate([scaled, jnp.zeros((112, 512), F32)], axis=0).T
    read_rows = []
    for n in range(16):
        column = turned[:, n : n + 1]
        if n >= HELD:
            loads[n - HELD].wait()
        if n < EARLY:
            source, at = early, n
        else:
            source, at = (held, n - EARLY) if n < HELD else (late, n - HELD)
        acc = jnp.zeros((8, 512), F32)
        for j in range(64):
            acc = acc + column[8 * j : 8 * j + 8] * source[at, 0, 8 * j : 8 * j + 8, :]
        read_rows.append(jnp.sum(acc, axis=0, keepdims=True))
    read = score * value + jnp.concatenate(read_rows, axis=0)
    centered = read - jnp.mean(read, axis=1, keepdims=True)
    gated = centered * rms_scale(centered) * hg[...] * jax.nn.sigmoid(outgate)
    out[...] = gated.astype(BF)


def read(own, came, gates, head_gain, early, held, memory):
    vmem = pl.BlockSpec(memory_space=pltpu.VMEM)
    late = memory.shape[0] - HELD
    return pl.pallas_call(
        read_kernel,
        in_specs=[vmem] * 8 + [pl.BlockSpec(memory_space=pltpu.HBM)],
        out_specs=vmem,
        out_shape=pltpu.VMEM((16, 512), BF),
        scratch_shapes=[
            pltpu.VMEM((late, *memory.shape[1:]), F32),
            pltpu.SemaphoreType.DMA((late,)),
        ],
        compiler_params=kernel_room(16),
        name="read",
    )(
        *on_chip(own, *came), gates, head_gain[None], early, held,
        pltpu.with_memory_space_constraint(memory, pltpu.HBM),
    )


def paired(mine, other, c, odd):
    first = jnp.where(c == 0, mine, other)
    second = jnp.where(c == 0, other, mine)
    low = lax.broadcasted_iota(jnp.int32, mine.shape, 1) < 64
    if odd:
        return jnp.where(low, pltpu.roll(first, 64, 1), second)
    return jnp.where(low, first, pltpu.roll(second, 64, 1))


def down_kernel(g, d0, d1, d2, d3, e0, e1, e2, e3, part, send, gains, factors):
    ep = lax.axis_index("ep")
    z, y, c = ep // (Y * C), (ep // C) & 3, ep & 1
    gated = g[...]
    for s, (d, e) in enumerate(zip((d0, d1, d2, d3), (e0, e1, e2, e3))):
        mine = lax.dot_general(gated, d[0:256], TURNED, preferred_element_type=F32)
        other = lax.dot_general(gated, e[0:256], TURNED, preferred_element_type=F32)
        my_gains = d[256:288, 0:128].astype(F32)
        other_gains = e[256:288, 0:128].astype(F32)
        for t in range(Y):
            at = slice(t // 2 * 128, t // 2 * 128 + 128)
            block = paired(mine[:, at], other[:, at], c, t % 2 == 1)
            off = pl.multiple_of(((z + (Z - s)) & 3) * 512 + ((y + (Y - t)) & 3) * 128, 128)
            part[:, pl.ds(off, 128)] = block
            send[:, pl.ds(off, 128)] = block.astype(BF)
            at = slice(8 * t, 8 * t + 8)
            factors[:, pl.ds(off, 128)] = paired(my_gains[at], other_gains[at], c, False)
    gains[0:1] = factors[0:1] + factors[1:2] + factors[2:3]
    gains[1:2] = factors[3:4] + factors[4:5] + factors[5:6]


def down_project(gated, own, partner):
    vmem = pl.BlockSpec(memory_space=pltpu.VMEM)
    return pl.pallas_call(
        down_kernel,
        in_specs=[vmem] * 9,
        out_specs=[vmem] * 3,
        out_shape=[
            pltpu.VMEM((16, 2048), F32),
            pltpu.VMEM((16, 2048), BF),
            pltpu.VMEM((8, 2048), F32),
        ],
        scratch_shapes=[pltpu.VMEM((8, 2048), F32)],
        compiler_params=kernel_room(8),
        name="down_project",
    )(gated, *on_chip(*own, *partner))


def fetch_experts_kernel(g, u, d, gate, up, down, sems):
    loads = [
        pltpu.make_async_copy(r.at[0], o, sems.at[i])
        for i, (r, o) in enumerate(((g, gate), (u, up), (d, down)))
    ]
    for load in loads:
        load.start()
    for load in loads:
        load.wait()


def fetch_experts(*arrays):
    return pl.pallas_call(
        fetch_experts_kernel,
        in_specs=[pl.BlockSpec(memory_space=pltpu.HBM)] * 3,
        out_specs=[pl.BlockSpec(memory_space=pltpu.VMEM)] * 3,
        out_shape=[pltpu.VMEM(a.shape[1:], BF) for a in arrays],
        scratch_shapes=[pltpu.SemaphoreType.DMA((3,))],
        compiler_params=kernel_room(4),
        name="fetch_experts",
    )(*[pltpu.with_memory_space_constraint(a, pltpu.HBM) for a in arrays])


def dispatch_kernel(x, part, r1, r2, r3, gains, send, residual, outgoing):
    mixed = part[...] + r1[...].astype(F32) + r2[...].astype(F32) + r3[...].astype(F32)
    total = x[...].astype(F32) + mixed * rms_scale(mixed) * gains[0:1]
    residual[...] = total.astype(BF)
    expert_in = (total * rms_scale(total) * gains[1:2]).astype(BF)
    halves = jnp.concatenate([expert_in[:, 0:1024], expert_in[:, 1024:2048]], axis=0)
    outgoing[...] = lax.dot_general(
        send[...], halves, (((0,), (0,)), ((), ())), preferred_element_type=F32
    ).astype(BF)


def dispatch(tokens, part, came, gains, send_from):
    vmem = pl.BlockSpec(memory_space=pltpu.VMEM)
    return pl.pallas_call(
        dispatch_kernel,
        in_specs=[vmem] * 7,
        out_specs=[vmem] * 2,
        out_shape=[pltpu.VMEM((16, 2048), BF), pltpu.VMEM((256, 1024), BF)],
        compiler_params=kernel_room(8),
        name="dispatch",
    )(tokens, part, *on_chip(*came), gains, send_from)


def experts_kernel(arrived, gate_w, up_w, down_w, out):
    row = lax.broadcasted_iota(jnp.int32, (128, 256), 0)
    lane = lax.broadcasted_iota(jnp.int32, (128, 256), 1)
    place = ((row >> 2) << 3) + (row & 3)
    rows = jnp.concatenate(
        [
            jnp.dot(
                jnp.where(lane == place + 4 * h, 1.0, 0.0).astype(BF), arrived[...],
                preferred_element_type=F32,
            ).astype(BF)
            for h in range(2)
        ],
        axis=1,
    )
    gate = jnp.minimum(jnp.dot(rows, gate_w[...], preferred_element_type=F32), CLAMP_LIMIT)
    up = jnp.clip(
        jnp.dot(rows, up_w[...], preferred_element_type=F32), -CLAMP_LIMIT, CLAMP_LIMIT
    )
    activation = ((up + 1.0) * gate * jax.nn.sigmoid(SIGMOID_SCALE * gate)).astype(BF)
    value = jnp.dot(activation, down_w[...], preferred_element_type=F32).astype(BF)
    both = jnp.concatenate([value[:, 0:1024], value[:, 1024:2048]], axis=0)
    goes = lax.broadcasted_iota(jnp.int32, (256, 256), 0)
    source = lax.broadcasted_iota(jnp.int32, (256, 256), 1)
    wanted = ((goes >> 2) & 1) * 128 + ((goes >> 3) << 2) + (goes & 3)
    out[...] = jnp.dot(
        jnp.where(source == wanted, 1.0, 0.0).astype(BF), both, preferred_element_type=F32
    ).astype(BF)


def run_experts(arrived, weights):
    vmem = pl.BlockSpec(memory_space=pltpu.VMEM)
    return pl.pallas_call(
        experts_kernel,
        in_specs=[vmem] * 4,
        out_specs=vmem,
        out_shape=pltpu.VMEM(arrived.shape, BF),
        compiler_params=kernel_room(16),
        name="experts",
    )(*on_chip(arrived), *weights)


def combine_kernel(take, returned, part, send):
    sums = jnp.dot(take[...], returned[...], preferred_element_type=F32)
    for h in range(2):
        at = 48 * h
        half = sums[at : at + 16] + sums[at + 16 : at + 32] + sums[at + 32 : at + 48]
        part[:, 1024 * h : 1024 * (h + 1)] = half
        send[:, 1024 * h : 1024 * (h + 1)] = half.astype(BF)


def combine(take_with, returned):
    vmem = pl.BlockSpec(memory_space=pltpu.VMEM)
    return pl.pallas_call(
        combine_kernel,
        in_specs=[vmem] * 2,
        out_specs=[vmem] * 2,
        out_shape=[pltpu.VMEM((16, 2048), F32), pltpu.VMEM((16, 2048), BF)],
        compiler_params=kernel_room(8),
        name="combine",
    )(take_with, *on_chip(returned))


def finish_kernel(part, r1, r2, r3, residual, gain, out, total):
    combined = part[...] + r1[...].astype(F32) + r2[...].astype(F32) + r3[...].astype(F32)
    scale = rms_scale(combined)
    total[...] = combined
    col = pl.multiple_of(lax.axis_index("tp") * 512, 128)
    mine = total[:, pl.ds(col, 512)]
    out[...] = (residual[:, pl.ds(col, 512)].astype(F32) + mine * scale * gain[...]).astype(BF)


def finish(part, came, residual, output_gain):
    vmem = pl.BlockSpec(memory_space=pltpu.VMEM)
    return pl.pallas_call(
        finish_kernel,
        in_specs=[vmem] * 6,
        out_specs=vmem,
        out_shape=jax.ShapeDtypeStruct((16, 512), BF),
        scratch_shapes=[pltpu.VMEM((16, 2048), F32)],
        compiler_params=kernel_room(8),
        name="finish",
    )(part, *on_chip(*came), residual, output_gain[None])


def layer(
    tokens,
    mixer_gain,
    query_weight,
    key_weight,
    value_weight,
    outgate_weight,
    igate_weight,
    fgate_weight,
    memory,
    stabilizer,
    head_gain,
    down_weight,
    mixed_gain,
    expert_gain,
    routes,
    route_weights,
    gate_proj,
    up_proj,
    expert_down,
    output_gain,
):
    ep_count = lax.axis_size("ep")
    *packed, gates, early = prepare(
        tokens, mixer_gain, down_weight, mixed_gain, expert_gain, igate_weight,
        fgate_weight, stabilizer, memory,
    )
    by_y = [packed[0]] + spread(lambda s: along_y(packed[s], s), FAR_FIRST)
    w0 = join((query_weight, key_weight, value_weight, outgate_weight))
    by_z = [w0] + spread(lambda s: along_z(w0, s), NEAR_FIRST)
    send_from, take_with = route(routes, route_weights)
    down_y = stack_down(by_y)
    down_z = [down_y] + spread(lambda s: along_z(down_y, s), NEAR_FIRST)
    held = fetch(memory, EARLY, HELD)
    partner = [other_core(w) for w in by_z]
    own, *owed = project(by_y, by_z, partner)
    came = spread(lambda s: along_y(owed[s - 1], -s), FAR_FIRST)
    down_partner = [other_core(d) for d in down_z[1:]]
    down_partner = [other_core(down_y)] + down_partner
    gated = read(own, came, gates, head_gain, early, held, memory)
    part, send, gains = down_project(gated, down_z, down_partner)
    mixed = spread(lambda s: along_tp(send, s), FAR_FIRST)
    weights = fetch_experts(gate_proj, up_proj, expert_down)
    residual, outgoing = dispatch(tokens, part, mixed, gains, send_from)
    arrived = lax.all_to_all(
        outgoing.reshape(ep_count, 8, 1024), "ep", 0, 0, tiled=True
    ).reshape(256, 1024)
    value = run_experts(arrived, weights)
    returned = lax.all_to_all(
        value.reshape(ep_count, 8, 1024), "ep", 0, 0, tiled=True
    ).reshape(256, 1024)
    own_sum, sent = combine(take_with, returned)
    others = spread(lambda s: along_tp(sent, s), FAR_FIRST)
    return finish(own_sum, others, residual, output_gain)


def solution(mesh):
    placed = (
        P("ep", None),
        P(),
        P("ep", "tp"),
        P("ep", "tp"),
        P("ep", "tp"),
        P("ep", "tp"),
        P("tp", None),
        P("tp", None),
        P("ep", "tp", None, None),
        P("ep", "tp"),
        P("tp"),
        P(None, "ep"),
        P("ep"),
        P("ep"),
        P(),
        P(),
        P("ep", None, "tp"),
        P("ep", None, "tp"),
        P("ep", "tp", None),
        P("tp"),
    )
    return jax.shard_map(
        layer, mesh=mesh, in_specs=placed, out_specs=P("ep", "tp"), check_vma=False
    )
```

```python
import jax
import jax.numpy as jnp
from jax import lax
from jax.experimental import pallas as pl
from jax.experimental.pallas import tpu as pltpu
from jax.sharding import PartitionSpec as P


NORM_EPS = 1e-06
CLAMP_LIMIT = 7.0
SIGMOID_SCALE = 1.702
BF = jnp.bfloat16
F32 = jnp.float32
Z, Y, C, TP = 4, 4, 2, 4
EARLY, HELD = 5, 13


def ep_at(z, y, c):
    return (z % Z) * (Y * C) + (y % Y) * C + c % C


def ep_moves(dz, dy, dc):
    return [
        (ep_at(z, y, c), ep_at(z + dz, y + dy, c + dc))
        for z in range(Z)
        for y in range(Y)
        for c in range(C)
    ]


def along_z(a, s):
    return lax.ppermute(a, "ep", ep_moves(s, 0, 0))


def along_y(a, s):
    return lax.ppermute(a, "ep", ep_moves(0, s, 0))


def spread(send, order):
    came = {}
    for s in order:
        came[s] = send(s)
    return [came[s] for s in (1, 2, 3)]


FAR_FIRST = (2, 1, 3)


def other_core(a):
    return lax.ppermute(a, "ep", ep_moves(0, 0, 1))


def along_tp(a, s):
    return lax.ppermute(a, "tp", [(i, (i + s) % TP) for i in range(TP)])


def on_chip(*arrays):
    return [pltpu.with_memory_space_constraint(a, pltpu.VMEM) for a in arrays]


def kernel_room(mebibytes):
    return pltpu.CompilerParams(vmem_limit_bytes=mebibytes << 20)


def rms_scale(values):
    return lax.rsqrt(jnp.mean(values * values, axis=-1, keepdims=True) + NORM_EPS)


def join_kernel(q, k, v, o, w0, sems):
    loads = [
        pltpu.make_async_copy(r, w0.at[:, pl.ds(i * 512, 512)], sems.at[i])
        for i, r in enumerate((q, k, v, o))
    ]
    for load in loads:
        load.start()
    for load in loads:
        load.wait()


def join(weights):
    return pl.pallas_call(
        join_kernel,
        in_specs=[pl.BlockSpec(memory_space=pl.ANY)] * 4,
        out_specs=pl.BlockSpec(memory_space=pltpu.VMEM),
        out_shape=pltpu.VMEM((64, 2048), BF),
        scratch_shapes=[pltpu.SemaphoreType.DMA((4,))],
        name="join",
    )(*weights)


def normed_of(x, gain):
    xf = x[...].astype(F32)
    return (xf * rms_scale(xf) * gain[...]).astype(BF)


def split_in_three(whole):
    high = whole.astype(BF).astype(F32)
    rest = whole - high
    mid = rest.astype(BF).astype(F32)
    return high, mid, rest - mid


TURNED = (((1,), (1,)), ((), ()))


def prepare_kernel(
    x_in, gain_in, dw, mg_in, eg_in, ig_in, fg_in, stab_in, memory,
    out0, out1, out2, out3, gates, early,
    x, gain, mg, eg, ig, fg, stab, normed, down, sems, row_sems,
):
    y = (lax.axis_index("ep") // C) & 3
    col = pl.multiple_of(lax.axis_index("tp") * 512, 128)
    pairs = (
        (x_in, x), (gain_in, gain), (mg_in, mg), (eg_in, eg), (ig_in, ig), (fg_in, fg),
        (stab_in, stab), (dw.at[:, pl.ds(col, 512)], down),
    )
    loads = [pltpu.make_async_copy(a, b, sems.at[i]) for i, (a, b) in enumerate(pairs)]
    rows = [
        pltpu.make_async_copy(memory.at[i], early.at[i], row_sems.at[i]) for i in range(EARLY)
    ]
    for load in loads + rows:
        load.start()
    for load in loads:
        load.wait()
    normed[...] = normed_of(x, gain)
    nf = normed[...].astype(F32)
    log_input = jnp.sum(nf * ig[...].astype(F32), axis=1, keepdims=True)
    pre = jnp.sum(nf * fg[...].astype(F32), axis=1, keepdims=True)
    log_forget = jnp.minimum(pre, 0.0) - jnp.log1p(jnp.exp(-jnp.abs(pre)))
    small = lax.broadcasted_iota(jnp.int32, (16, 16), 0)
    across = lax.broadcasted_iota(jnp.int32, (16, 16), 1)
    stab_column = jnp.sum(jnp.where(small == across, stab[...], 0.0), axis=1, keepdims=True)
    first = lax.broadcasted_iota(jnp.int32, (16, 128), 1)
    gates[...] = jnp.where(first == 0, log_input, log_forget + stab_column)
    row = lax.broadcasted_iota(jnp.int32, (8, 64), 0)
    extra = jnp.zeros((8, 64), F32)
    for i, g in enumerate((mg, eg)):
        for j, piece in enumerate(split_in_three(g[...])):
            extra = jnp.where(row == 3 * i + j, piece, extra)
    extra = jnp.concatenate([extra, jnp.zeros((8, 576), F32)], axis=1).astype(BF)
    for s, out in enumerate((out0, out1, out2, out3)):
        out[0:64, 0:512] = down[...]
        out[64:72] = extra
        target = (y + s) & 3
        for i in range(Z):
            off = pl.multiple_of(512 * i + target * 128, 128)
            out[16 * i : 16 * i + 16, 512:640] = normed[:, pl.ds(off, 128)]
    for load in rows:
        load.wait()


def prepare(tokens, mixer_gain, down_weight, mg, eg, ig, fg, stabilizer, memory):
    vmem = pl.BlockSpec(memory_space=pltpu.VMEM)
    ins = [tokens, mixer_gain[None], down_weight.T, mg[None], eg[None], ig, fg, stabilizer.T]
    ins = [pltpu.with_memory_space_constraint(a, pltpu.HBM) for a in ins + [memory]]
    return pl.pallas_call(
        prepare_kernel,
        in_specs=[pl.BlockSpec(memory_space=pltpu.HBM)] * 9,
        out_specs=[vmem] * 6,
        out_shape=[pltpu.VMEM((72, 640), BF)] * 4
        + [pltpu.VMEM((16, 128), F32), pltpu.VMEM((EARLY, *memory.shape[1:]), F32)],
        scratch_shapes=[pltpu.VMEM(ins[i].shape, ins[i].dtype) for i in (0, 1, 3, 4, 5, 6, 7)]
        + [
            pltpu.VMEM((16, 2048), BF),
            pltpu.VMEM((64, 512), BF),
            pltpu.SemaphoreType.DMA((8,)),
            pltpu.SemaphoreType.DMA((EARLY,)),
        ],
        compiler_params=kernel_room(4),
        name="prepare",
    )(*ins)


def route_kernel(routes, weights, send, take):
    small = lax.broadcasted_iota(jnp.int32, (16, 16), 0)
    across = lax.broadcasted_iota(jnp.int32, (16, 16), 1)
    pick = jnp.where(
        lax.broadcasted_iota(jnp.int32, (16, 512), 1)
        == lax.broadcasted_iota(jnp.int32, (16, 512), 0) + lax.axis_index("ep") * 16,
        1.0,
        0.0,
    )
    chosen = lax.dot_general(
        pick, routes[...].astype(F32), TURNED, precision=lax.Precision.HIGHEST,
        preferred_element_type=F32,
    )
    weight = lax.dot_general(
        pick, weights[...], TURNED, precision=lax.Precision.HIGHEST, preferred_element_type=F32
    )
    lane = lax.broadcasted_iota(jnp.int32, (16, 256), 1)
    expert_of = (lane >> 3).astype(F32)
    named = jnp.zeros((16, 256), F32)
    weight_of = jnp.zeros((16, 256), F32)
    for k in range(4):
        hit = chosen[:, k : k + 1] == expert_of
        named = jnp.where(hit, 1.0, named)
        weight_of = jnp.where(hit, weight[:, k : k + 1], weight_of)
    before = jnp.dot(
        jnp.where(small > across, 1.0, 0.0).astype(BF), named.astype(BF),
        preferred_element_type=F32,
    )
    placed = (named > 0.5) & (before == (lane & 3).astype(F32))
    for h in range(2):
        half = placed & (((lane >> 2) & 1) == h)
        send[16 * h : 16 * h + 16] = jnp.where(half, 1.0, 0.0).astype(BF)
        taken = jnp.where(half, weight_of, 0.0)
        for j, piece in enumerate(split_in_three(taken)):
            at = 48 * h + 16 * j
            take[at : at + 16] = piece.astype(BF)


def route(routes, weights):
    vmem = pl.BlockSpec(memory_space=pltpu.VMEM)
    return pl.pallas_call(
        route_kernel,
        in_specs=[vmem] * 2,
        out_specs=[vmem] * 2,
        out_shape=[
            pltpu.VMEM((32, 256), BF),
            pltpu.VMEM((96, 256), BF),
        ],
        compiler_params=kernel_room(4),
        name="route",
    )(routes.T, weights.T)


def stack_kernel(a0, a1, a2, a3, out):
    gains = jnp.zeros((8, 256), F32)
    for i, a in enumerate((a0, a1, a2, a3)):
        out[64 * i : 64 * i + 64] = a[0:64, 0:512]
        piece = a[64:72, 0:256].astype(F32)
        gains = gains + (pltpu.roll(piece, 64 * i, 1) if i else piece)
    out[256:264, 0:256] = gains.astype(BF)
    out[256:264, 256:512] = jnp.zeros((8, 256), BF)


def stack_down(pieces):
    vmem = pl.BlockSpec(memory_space=pltpu.VMEM)
    return pl.pallas_call(
        stack_kernel,
        in_specs=[vmem] * 4,
        out_specs=vmem,
        out_shape=pltpu.VMEM((264, 512), BF),
        compiler_params=kernel_room(4),
        name="stack_down",
    )(*on_chip(*pieces))


def project_kernel(
    n0, n1, n2, n3, w0, w1, w2, w3, p0, p1, p2, p3, own, t1, t2, t3
):
    ep = lax.axis_index("ep")
    z, c = ep // (Y * C), ep & 1
    rows = []
    for n in (n0, n1, n2, n3):
        chunks = []
        for s in range(Z):
            off = pl.multiple_of(((z + (Z - s)) & 3) * 16, 16)
            part = n[pl.ds(off, 16), 512:640].astype(F32)
            chunks.append(jnp.where(c == 0, part, pltpu.roll(part, 64, 1)).astype(BF))
        rows.append(jnp.concatenate(chunks, axis=1))
    x = jnp.concatenate(rows, axis=0)
    pieces = [r for pair in zip((w0, w1, w2, w3), (p0, p1, p2, p3)) for r in pair]
    for i in range(4):
        at_i = slice(512 * i, 512 * (i + 1))
        w = jnp.concatenate([r[:, at_i] for r in pieces], axis=0)
        acc = jnp.dot(x, w, preferred_element_type=F32)
        own[:, at_i] = acc[0:16]
        for k, t in ((16, t1), (32, t2), (48, t3)):
            part = acc[k : k + 16]
            high = part.astype(BF)
            t[:, at_i] = high
            if i < 2:
                low = (part - high.astype(F32)).astype(BF)
                t[:, 2048 + 512 * i : 2048 + 512 * (i + 1)] = low


def project(packed_by_shift, weights, partner):
    rows, width = 16, weights[0].shape[1]
    vmem = pl.BlockSpec(memory_space=pltpu.VMEM)
    return pl.pallas_call(
        project_kernel,
        in_specs=[vmem] * 12,
        out_specs=[vmem] * 4,
        out_shape=[pltpu.VMEM((rows, width), F32)]
        + [pltpu.VMEM((rows, width + width // 2), BF)] * 3,
        compiler_params=kernel_room(8),
        name="project",
    )(*on_chip(*packed_by_shift, *weights, *partner))


def fetch(memory, start, stop):
    def kernel(whole, out, sems):
        loads = [
            pltpu.make_async_copy(whole.at[start + i], out.at[i], sems.at[i])
            for i in range(stop - start)
        ]
        for load in loads:
            load.start()
        for load in loads:
            load.wait()

    return pl.pallas_call(
        kernel,
        in_specs=[pl.BlockSpec(memory_space=pltpu.HBM)],
        out_specs=pl.BlockSpec(memory_space=pltpu.VMEM),
        out_shape=pltpu.VMEM((stop - start, *memory.shape[1:]), F32),
        scratch_shapes=[pltpu.SemaphoreType.DMA((stop - start,))],
        compiler_params=kernel_room(4),
        name="fetch_rows",
    )(pltpu.with_memory_space_constraint(memory, pltpu.HBM))


def read_kernel(own, r1, r2, r3, gates, hg, early, held, memory, out, late, sems):
    loads = [
        pltpu.make_async_copy(memory.at[HELD + i], late.at[i], sems.at[i])
        for i in range(late.shape[0])
    ]
    for load in loads:
        load.start()
    parts = []
    for i in range(4):
        at_i = slice(512 * i, 512 * (i + 1))
        total = own[:, at_i]
        for r in (r1, r2, r3):
            came = r[:, at_i].astype(F32)
            if i < 2:
                came = came + r[:, 2048 + 512 * i : 2048 + 512 * (i + 1)].astype(F32)
            total = total + came
        parts.append(total.astype(BF).astype(F32))
    query, key, value, outgate = parts
    query = query * 512 ** (-0.5)
    log_input, carry = gates[:, 0:1], gates[:, 1:2]
    peak = jnp.maximum(carry, log_input)
    within = jnp.exp(log_input - peak)
    carried = jnp.exp(carry - peak)
    score = jnp.sum(query * key, axis=1, keepdims=True) * within
    scaled = query * carried
    turned = jnp.concatenate([scaled, jnp.zeros((112, 512), F32)], axis=0).T
    read_rows = []
    for n in range(16):
        column = turned[:, n : n + 1]
        if n >= HELD:
            loads[n - HELD].wait()
        if n < EARLY:
            source, at = early, n
        else:
            source, at = (held, n - EARLY) if n < HELD else (late, n - HELD)
        acc = jnp.zeros((8, 512), F32)
        for j in range(64):
            acc = acc + column[8 * j : 8 * j + 8] * source[at, 0, 8 * j : 8 * j + 8, :]
        read_rows.append(jnp.sum(acc, axis=0, keepdims=True))
    read = score * value + jnp.concatenate(read_rows, axis=0)
    centered = read - jnp.mean(read, axis=1, keepdims=True)
    gated = centered * rms_scale(centered) * hg[...] * jax.nn.sigmoid(outgate)
    out[...] = gated.astype(BF)


def read(own, came, gates, head_gain, early, held, memory):
    vmem = pl.BlockSpec(memory_space=pltpu.VMEM)
    late = memory.shape[0] - HELD
    return pl.pallas_call(
        read_kernel,
        in_specs=[vmem] * 8 + [pl.BlockSpec(memory_space=pltpu.HBM)],
        out_specs=vmem,
        out_shape=pltpu.VMEM((16, 512), BF),
        scratch_shapes=[
            pltpu.VMEM((late, *memory.shape[1:]), F32),
            pltpu.SemaphoreType.DMA((late,)),
        ],
        compiler_params=kernel_room(16),
        name="read",
    )(
        *on_chip(own, *came), gates, head_gain[None], early, held,
        pltpu.with_memory_space_constraint(memory, pltpu.HBM),
    )


def paired(mine, other, c, odd):
    first = jnp.where(c == 0, mine, other)
    second = jnp.where(c == 0, other, mine)
    low = lax.broadcasted_iota(jnp.int32, mine.shape, 1) < 64
    if odd:
        return jnp.where(low, pltpu.roll(first, 64, 1), second)
    return jnp.where(low, first, pltpu.roll(second, 64, 1))


def down_kernel(g, d0, d1, d2, d3, e0, e1, e2, e3, part, send, gains, factors):
    ep = lax.axis_index("ep")
    z, y, c = ep // (Y * C), (ep // C) & 3, ep & 1
    gated = g[...]
    for s, (d, e) in enumerate(zip((d0, d1, d2, d3), (e0, e1, e2, e3))):
        mine = lax.dot_general(gated, d[0:256], TURNED, preferred_element_type=F32)
        other = lax.dot_general(gated, e[0:256], TURNED, preferred_element_type=F32)
        my_gains = d[256:264, 0:256].astype(F32)
        other_gains = e[256:264, 0:256].astype(F32)
        for t in range(Y):
            at = slice(t // 2 * 128, t // 2 * 128 + 128)
            block = paired(mine[:, at], other[:, at], c, t % 2 == 1)
            off = pl.multiple_of(((z + (Z - s)) & 3) * 512 + ((y + (Y - t)) & 3) * 128, 128)
            part[:, pl.ds(off, 128)] = block
            send[:, pl.ds(off, 128)] = block.astype(BF)
            factors[:, pl.ds(off, 128)] = paired(my_gains[:, at], other_gains[:, at], c, t % 2 == 1)
    gains[0:1] = factors[0:1] + factors[1:2] + factors[2:3]
    gains[1:2] = factors[3:4] + factors[4:5] + factors[5:6]


def down_project(gated, own, partner):
    vmem = pl.BlockSpec(memory_space=pltpu.VMEM)
    return pl.pallas_call(
        down_kernel,
        in_specs=[vmem] * 9,
        out_specs=[vmem] * 3,
        out_shape=[
            pltpu.VMEM((16, 2048), F32),
            pltpu.VMEM((16, 2048), BF),
            pltpu.VMEM((8, 2048), F32),
        ],
        scratch_shapes=[pltpu.VMEM((8, 2048), F32)],
        compiler_params=kernel_room(8),
        name="down_project",
    )(gated, *on_chip(*own, *partner))


def fetch_experts_kernel(g, u, d, gate, up, down, sems):
    loads = [
        pltpu.make_async_copy(r.at[0], o, sems.at[i])
        for i, (r, o) in enumerate(((g, gate), (u, up), (d, down)))
    ]
    for load in loads:
        load.start()
    for load in loads:
        load.wait()


def fetch_experts(*arrays):
    return pl.pallas_call(
        fetch_experts_kernel,
        in_specs=[pl.BlockSpec(memory_space=pltpu.HBM)] * 3,
        out_specs=[pl.BlockSpec(memory_space=pltpu.VMEM)] * 3,
        out_shape=[pltpu.VMEM(a.shape[1:], BF) for a in arrays],
        scratch_shapes=[pltpu.SemaphoreType.DMA((3,))],
        compiler_params=kernel_room(4),
        name="fetch_experts",
    )(*[pltpu.with_memory_space_constraint(a, pltpu.HBM) for a in arrays])


def dispatch_kernel(x, part, r1, r2, r3, gains, send, residual, outgoing):
    mixed = part[...] + r1[...].astype(F32) + r2[...].astype(F32) + r3[...].astype(F32)
    total = x[...].astype(F32) + mixed * rms_scale(mixed) * gains[0:1]
    residual[...] = total.astype(BF)
    expert_in = (total * rms_scale(total) * gains[1:2]).astype(BF)
    halves = jnp.concatenate([expert_in[:, 0:1024], expert_in[:, 1024:2048]], axis=0)
    outgoing[...] = lax.dot_general(
        send[...], halves, (((0,), (0,)), ((), ())), preferred_element_type=F32
    ).astype(BF)


def dispatch(tokens, part, came, gains, send_from):
    vmem = pl.BlockSpec(memory_space=pltpu.VMEM)
    return pl.pallas_call(
        dispatch_kernel,
        in_specs=[vmem] * 7,
        out_specs=[vmem] * 2,
        out_shape=[pltpu.VMEM((16, 2048), BF), pltpu.VMEM((256, 1024), BF)],
        compiler_params=kernel_room(8),
        name="dispatch",
    )(tokens, part, *on_chip(*came), gains, send_from)


def experts_kernel(arrived, gate_w, up_w, down_w, out):
    row = lax.broadcasted_iota(jnp.int32, (128, 256), 0)
    lane = lax.broadcasted_iota(jnp.int32, (128, 256), 1)
    place = ((row >> 2) << 3) + (row & 3)
    rows = jnp.concatenate(
        [
            jnp.dot(
                jnp.where(lane == place + 4 * h, 1.0, 0.0).astype(BF), arrived[...],
                preferred_element_type=F32,
            ).astype(BF)
            for h in range(2)
        ],
        axis=1,
    )
    gate = jnp.minimum(jnp.dot(rows, gate_w[...], preferred_element_type=F32), CLAMP_LIMIT)
    up = jnp.clip(
        jnp.dot(rows, up_w[...], preferred_element_type=F32), -CLAMP_LIMIT, CLAMP_LIMIT
    )
    activation = ((up + 1.0) * gate * jax.nn.sigmoid(SIGMOID_SCALE * gate)).astype(BF)
    value = jnp.dot(activation, down_w[...], preferred_element_type=F32).astype(BF)
    both = jnp.concatenate([value[:, 0:1024], value[:, 1024:2048]], axis=0)
    goes = lax.broadcasted_iota(jnp.int32, (256, 256), 0)
    source = lax.broadcasted_iota(jnp.int32, (256, 256), 1)
    wanted = ((goes >> 2) & 1) * 128 + ((goes >> 3) << 2) + (goes & 3)
    out[...] = jnp.dot(
        jnp.where(source == wanted, 1.0, 0.0).astype(BF), both, preferred_element_type=F32
    ).astype(BF)


def run_experts(arrived, weights):
    vmem = pl.BlockSpec(memory_space=pltpu.VMEM)
    return pl.pallas_call(
        experts_kernel,
        in_specs=[vmem] * 4,
        out_specs=vmem,
        out_shape=pltpu.VMEM(arrived.shape, BF),
        compiler_params=kernel_room(16),
        name="experts",
    )(*on_chip(arrived), *weights)


def combine_kernel(take, returned, part, send):
    sums = jnp.dot(take[...], returned[...], preferred_element_type=F32)
    for h in range(2):
        at = 48 * h
        half = sums[at : at + 16] + sums[at + 16 : at + 32] + sums[at + 32 : at + 48]
        part[:, 1024 * h : 1024 * (h + 1)] = half
        send[:, 1024 * h : 1024 * (h + 1)] = half.astype(BF)


def combine(take_with, returned):
    vmem = pl.BlockSpec(memory_space=pltpu.VMEM)
    return pl.pallas_call(
        combine_kernel,
        in_specs=[vmem] * 2,
        out_specs=[vmem] * 2,
        out_shape=[pltpu.VMEM((16, 2048), F32), pltpu.VMEM((16, 2048), BF)],
        compiler_params=kernel_room(8),
        name="combine",
    )(take_with, *on_chip(returned))


def finish_kernel(part, r1, r2, r3, residual, gain, out, total):
    combined = part[...] + r1[...].astype(F32) + r2[...].astype(F32) + r3[...].astype(F32)
    scale = rms_scale(combined)
    total[...] = combined
    col = pl.multiple_of(lax.axis_index("tp") * 512, 128)
    mine = total[:, pl.ds(col, 512)]
    out[...] = (residual[:, pl.ds(col, 512)].astype(F32) + mine * scale * gain[...]).astype(BF)


def finish(part, came, residual, output_gain):
    vmem = pl.BlockSpec(memory_space=pltpu.VMEM)
    return pl.pallas_call(
        finish_kernel,
        in_specs=[vmem] * 6,
        out_specs=vmem,
        out_shape=jax.ShapeDtypeStruct((16, 512), BF),
        scratch_shapes=[pltpu.VMEM((16, 2048), F32)],
        compiler_params=kernel_room(8),
        name="finish",
    )(part, *on_chip(*came), residual, output_gain[None])


def layer(
    tokens,
    mixer_gain,
    query_weight,
    key_weight,
    value_weight,
    outgate_weight,
    igate_weight,
    fgate_weight,
    memory,
    stabilizer,
    head_gain,
    down_weight,
    mixed_gain,
    expert_gain,
    routes,
    route_weights,
    gate_proj,
    up_proj,
    expert_down,
    output_gain,
):
    ep_count = lax.axis_size("ep")
    *packed, gates, early = prepare(
        tokens, mixer_gain, down_weight, mixed_gain, expert_gain, igate_weight,
        fgate_weight, stabilizer, memory,
    )
    by_y = [packed[0]] + spread(lambda s: along_y(packed[s], s), FAR_FIRST)
    w0 = join((query_weight, key_weight, value_weight, outgate_weight))
    by_z = [w0] + spread(lambda s: along_z(w0, s), FAR_FIRST)
    send_from, take_with = route(routes, route_weights)
    down_y = stack_down(by_y)
    down_z = [down_y] + spread(lambda s: along_z(down_y, s), FAR_FIRST)
    held = fetch(memory, EARLY, HELD)
    own_partner = other_core(w0)
    partner = [own_partner] + spread(lambda s: other_core(by_z[s]), FAR_FIRST)
    own, *owed = project(by_y, by_z, partner)
    came = spread(lambda s: along_y(owed[s - 1], -s), FAR_FIRST)
    down_partner = spread(lambda s: other_core(down_z[s]), FAR_FIRST)
    down_partner = [other_core(down_y)] + down_partner
    gated = read(own, came, gates, head_gain, early, held, memory)
    part, send, gains = down_project(gated, down_z, down_partner)
    mixed = spread(lambda s: along_tp(send, s), FAR_FIRST)
    weights = fetch_experts(gate_proj, up_proj, expert_down)
    residual, outgoing = dispatch(tokens, part, mixed, gains, send_from)
    arrived = lax.all_to_all(
        outgoing.reshape(ep_count, 8, 1024), "ep", 0, 0, tiled=True
    ).reshape(256, 1024)
    value = run_experts(arrived, weights)
    returned = lax.all_to_all(
        value.reshape(ep_count, 8, 1024), "ep", 0, 0, tiled=True
    ).reshape(256, 1024)
    own_sum, sent = combine(take_with, returned)
    others = spread(lambda s: along_tp(sent, s), FAR_FIRST)
    return finish(own_sum, others, residual, output_gain)


def solution(mesh):
    placed = (
        P("ep", None),
        P(),
        P("ep", "tp"),
        P("ep", "tp"),
        P("ep", "tp"),
        P("ep", "tp"),
        P("tp", None),
        P("tp", None),
        P("ep", "tp", None, None),
        P("ep", "tp"),
        P("tp"),
        P(None, "ep"),
        P("ep"),
        P("ep"),
        P(),
        P(),
        P("ep", None, "tp"),
        P("ep", None, "tp"),
        P("ep", "tp", None),
        P("tp"),
    )
    return jax.shard_map(
        layer, mesh=mesh, in_specs=placed, out_specs=P("ep", "tp"), check_vma=False
    )
```
